512 devices in a mesh: sp: 64 (over z, y), tp: 8 (over x, core).
Axes of the slice: x: 4, y: 4, z: 16, core: 2. Of those that a mesh axis runs over, the one named last changes fastest.
Arguments:
- query_logits: bfloat16 [8192, 1024], P('sp', 'tp'), may hold values from -6 to 6
- value_rows: bfloat16 [8192, 1024], P('sp', 'tp'), may hold values from -6 to 6
- onward_forget_logits: bfloat16 [8192, 1024], P('sp', 'tp'), may hold values from -5.5 to 5.5
- reverse_forget_logits: bfloat16 [8192, 1024], P('sp', 'tp'), may hold values from -5.5 to 5.5
- output_gate_logits: bfloat16 [8192, 1024], P('sp', 'tp'), may hold values from -6 to 6
- onward_floor_gap: float32 [1024], P('tp'), may hold values from 0 to 0.12, as said below
- reverse_floor_gap: float32 [1024], P('tp'), may hold values from 0 to 0.12, as said below
- extra_log_decay: float32 [8192, 8], P('sp', 'tp'), may hold values from -2.1 to 0
- per_head_gain: float32 [128], replicated, may hold values from 0.1 to 1.9
- residual: bfloat16 [8192, 2048], P('sp', 'tp'), may hold values from -8 to 8
- output_matrix: bfloat16 [1024, 2048], P(None, 'tp'), may hold values from -0.375 to 0.375
- inner_norm_gain: float32 [2048], P('tp'), may hold values from 0.1 to 1.9
- inner_norm_bias: float32 [2048], P('tp'), may hold values from -1.5 to 1.5
- gate_matrix: bfloat16 [2048, 5632], P('sp', 'tp'), may hold values from -0.125 to 0.125
- up_matrix: bfloat16 [2048, 5632], P('sp', 'tp'), may hold values from -0.125 to 0.125
- down_matrix: bfloat16 [5632, 2048], P('tp', 'sp'), may hold values from -0.15625 to 0.15625
- closing_norm_gain: float32 [2048], P('tp'), may hold values from 0.1 to 1.9
- closing_norm_bias: float32 [2048], P('tp'), may hold values from -1.5 to 1.5
Outputs:
- layer_output: bfloat16 [8192, 2048], P('sp', 'tp')
The draws below stay inside these ranges and needn't reach their ends.
Inputs may be any that keep to these rules, and one draw needn't show every extreme that they name: `onward_floor_gap`: positive. `reverse_floor_gap`: positive.
All inputs are finite; a program needn't handle non-finite values.
Results may differ from the reference program's by a relative error of at most 0.014.
Values may be sent and summed in bfloat16 or wider, within the bound.
No kernel may reach another device: no remote copies, remote signals or barrier semaphores. Data moves between devices by JAX's collectives and lax.ppermute only.
A program may use at most 64 MiB of HBM per device.

```python
import math
import jax
import jax.numpy as jnp
from jax import lax

D = 2048
HEADS = 8
HEAD_WIDTH = 128
FF = 5632
TOK_DEV = 128
TOKENS = 8192
N_TP = 8


def forget_values(key):
    block_shift = jax.random.uniform(jax.random.fold_in(key, 11), (TOKENS // TOK_DEV, 1), jnp.float32, -1.5, 1.5)
    shift = jnp.repeat(block_shift, TOK_DEV, axis=0)
    noise = jnp.clip(jax.random.normal(key, (TOKENS, HEADS * HEAD_WIDTH), jnp.float32), -4.0, 4.0)
    return (noise + shift).astype(jnp.bfloat16)


def floor_values(key):
    order = jax.random.permutation(jax.random.fold_in(key, 1), HEADS)
    fast = order < HEADS // 2
    quick = jax.random.uniform(jax.random.fold_in(key, 2), (HEADS, HEAD_WIDTH), jnp.float32, 0.03, 0.12)
    slow = jax.random.uniform(jax.random.fold_in(key, 3), (HEADS, HEAD_WIDTH), jnp.float32, 0.3, 1.2) / TOKENS
    return jnp.where(fast[:, None], quick, slow).reshape(HEADS * HEAD_WIDTH).astype(jnp.float32)


def draw_onward_forget_logits(key, part):
    return forget_values(jax.random.fold_in(key, 101))


def draw_reverse_forget_logits(key, part):
    return forget_values(jax.random.fold_in(key, 202))


def draw_onward_floor_gap(key, part):
    return floor_values(jax.random.fold_in(key, 303))


def draw_reverse_floor_gap(key, part):
    return floor_values(jax.random.fold_in(key, 404))


def draw_extra_log_decay(key, part):
    inner = jax.random.fold_in(key, 505)
    spots = jax.random.randint(jax.random.fold_in(inner, 1), (3, HEADS), 0, TOKENS)
    depth = jnp.log(jax.random.uniform(jax.random.fold_in(inner, 2), (3, HEADS), jnp.float32, 0.5, 0.8))
    places = jnp.arange(TOKENS, dtype=jnp.int32)[:, None, None] == spots[None]
    return jnp.sum(jnp.where(places, depth[None], 0.0), axis=1).astype(jnp.float32)


def draw_residual(key, part):
    inner = jax.random.fold_in(key, 606)
    ramp = 0.6 + 1.2 * jnp.arange(D, dtype=jnp.float32) / D
    base = jax.random.normal(inner, (TOKENS, D), jnp.float32)
    return jnp.clip(base * ramp, -8.0, 8.0).astype(jnp.bfloat16)


def shard_levels(stream_key, extent, pieces, smallest, largest):
    def one(dim, shards_of):
        steps = jax.random.uniform(jax.random.fold_in(jax.random.fold_in(stream_key, 6), dim), (shards_of,), jnp.float32, smallest / len(pieces), largest / len(pieces))
        return jnp.repeat(jnp.exp(steps), extent[dim] // shards_of).reshape((-1,) + (1,) * (len(extent) - dim - 1))

    level = one(*pieces[0])
    for cut in pieces[1:]:
        level = level * one(*cut)
    return level


def bell_draw(key, shape, scale, limit, cuts=(), kind=jnp.bfloat16):
    level = shard_levels(key, shape, cuts, -0.22, 0.18) if cuts else 1.0
    values = jax.random.normal(key, shape, jnp.float32) * scale * level
    return jnp.minimum(jnp.maximum(values, -limit), limit).astype(kind)


def setup_inputs(seed: int = 0) -> dict:
    arg_keys = jax.random.split(jax.random.key(seed), 19)
    return {
        "query_logits": bell_draw(arg_keys[0], (TOKENS, HEADS * HEAD_WIDTH), 1.0, 6.0, ((0, 64), (1, 8))),
        "value_rows": bell_draw(arg_keys[1], (TOKENS, HEADS * HEAD_WIDTH), 1.0, 6.0, ((0, 64), (1, 8))),
        "onward_forget_logits": draw_onward_forget_logits(jax.random.fold_in(arg_keys[18], 71), 0),
        "reverse_forget_logits": draw_reverse_forget_logits(jax.random.fold_in(arg_keys[18], 71), 0),
        "output_gate_logits": bell_draw(arg_keys[4], (TOKENS, HEADS * HEAD_WIDTH), 1.0, 6.0, ((0, 64), (1, 8))),
        "onward_floor_gap": draw_onward_floor_gap(jax.random.fold_in(arg_keys[18], 71), 0),
        "reverse_floor_gap": draw_reverse_floor_gap(jax.random.fold_in(arg_keys[18], 71), 0),
        "extra_log_decay": draw_extra_log_decay(jax.random.fold_in(arg_keys[18], 71), 0),
        "per_head_gain": jnp.clip(1.0 + 0.18 * jax.random.normal(arg_keys[8], (HEAD_WIDTH,), jnp.float32), 0.1, 1.9),
        "residual": draw_residual(jax.random.fold_in(arg_keys[18], 71), 0),
        "output_matrix": bell_draw(arg_keys[10], (HEADS * HEAD_WIDTH, D), (HEADS * HEAD_WIDTH // 4) ** -0.5, 0.375, ((1, 8),)),
        "inner_norm_gain": jnp.clip(1.0 + 0.18 * jax.random.normal(arg_keys[11], (D,), jnp.float32), 0.1, 1.9),
        "inner_norm_bias": bell_draw(arg_keys[12], (D,), 0.3, 1.5, ((0, 8),), jnp.float32),
        "gate_matrix": bell_draw(arg_keys[13], (D, FF), D ** -0.5, 0.125, ((0, 64), (1, 8))),
        "up_matrix": bell_draw(arg_keys[14], (D, FF), D ** -0.5, 0.125, ((0, 64), (1, 8))),
        "down_matrix": bell_draw(arg_keys[15], (FF, D), (FF // 4) ** -0.5, 0.15625, ((0, 8), (1, 64))),
        "closing_norm_gain": jnp.clip(1.0 + 0.18 * jax.random.normal(arg_keys[16], (D,), jnp.float32), 0.1, 1.9),
        "closing_norm_bias": bell_draw(arg_keys[17], (D,), 0.3, 1.5, ((0, 8),), jnp.float32),
    }


highest_precision = lax.Precision.HIGHEST
alpha_mix = 2.0 ** 0.25
norm_eps = 1e-05
head_eps = 1e-06

def decay_factors(unscaled_input, lower_bound_gap, extra_decays):
    decay_factor = lower_bound_gap * jax.nn.sigmoid(-unscaled_input.astype(jnp.float32))
    return (jnp.log1p(-decay_factor) + extra_decays, decay_factor)

def recurrence(query, keys, values, log_decay):
    total, head_count, model_width = query.shape
    span = math.gcd(total, 128)
    count = total // span
    triangle = jnp.tril(jnp.ones((span, span), jnp.float32))

    def blocks(array):
        return array.reshape(count, span, head_count, array.shape[2])

    def advance(running_state, inputs):
        query_block, key_block, value_tile, log_block = inputs
        running = jnp.cumsum(log_block, axis=0)
        final_index = running[-1]
        decayed_query = query_block * jnp.exp(running)
        key_inverse = key_block * jnp.exp(-running)
        key_stop = key_block * jnp.exp(final_index[None] - running)
        scores = jnp.einsum('thk,shk->hts', decayed_query, key_inverse, precision=highest_precision) * triangle[None]
        inner = jnp.einsum('hts,shv->thv', scores, value_tile, precision=highest_precision)
        carried_state = jnp.einsum('nex,exl->nel', decayed_query, running_state, precision=highest_precision)
        running_state = jnp.exp(final_index)[:, :, None] * running_state + jnp.einsum('ojy,oje->jye', key_stop, value_tile, precision=highest_precision)
        return (running_state, inner + carried_state)
    start = jnp.zeros((head_count, model_width, values.shape[2]), jnp.float32)
    final, outputs = lax.scan(advance, start, (blocks(query), blocks(keys), blocks(values), blocks(log_decay)))
    return outputs.reshape(total, head_count, values.shape[2])

def layer_norm(rows, gain, bias):
    centre = rows - lax.optimization_barrier(jnp.mean(rows, axis=-1, keepdims=True))
    spread = lax.optimization_barrier(jnp.mean(centre * centre, axis=-1, keepdims=True))
    return centre * lax.rsqrt(spread + norm_eps) * gain + bias

def reference(query_logits, value_rows, onward_forget_logits, reverse_forget_logits, output_gate_logits, onward_floor_gap, reverse_floor_gap, extra_log_decay, per_head_gain, residual, output_matrix, inner_norm_gain, inner_norm_bias, gate_matrix, up_matrix, down_matrix, closing_norm_gain, closing_norm_bias):
    total = query_logits.shape[0]
    shape_head = (total, HEADS, HEAD_WIDTH)
    query = jax.nn.silu(query_logits.astype(jnp.float32)).reshape(shape_head)
    values = value_rows.astype(jnp.float32).reshape(shape_head)
    extra_decays = jnp.repeat(extra_log_decay, HEAD_WIDTH, axis=1)
    onward_log_decay, onward_key_rows = decay_factors(onward_forget_logits, onward_floor_gap, extra_decays)
    reverse_log_decay, reverse_key_rows = decay_factors(reverse_forget_logits, reverse_floor_gap, extra_decays)
    upcoming_part = recurrence(query, onward_key_rows.reshape(shape_head), values, onward_log_decay.reshape(shape_head))
    preceding_part = jnp.flip(recurrence(jnp.flip(query, axis=0), jnp.flip(reverse_key_rows.reshape(shape_head), axis=0), jnp.flip(values, axis=0), jnp.flip(reverse_log_decay.reshape(shape_head), axis=0)), axis=0)
    mixed = upcoming_part + preceding_part
    normed = mixed * lax.rsqrt(lax.optimization_barrier(jnp.mean(mixed * mixed, axis=2, keepdims=True)) + head_eps) * per_head_gain
    gated = (normed.reshape(total, HEADS * HEAD_WIDTH) * jax.nn.silu(output_gate_logits.astype(jnp.float32))).astype(jnp.bfloat16)
    piece_rows = math.gcd(total, 2048)
    count = total // piece_rows
    share = FF // N_TP

    def finish(inputs):
        gated_rows, residual_rows = inputs
        mixer = jnp.dot(gated_rows, output_matrix, preferred_element_type=jnp.float32)
        middle = layer_norm(alpha_mix * residual_rows.astype(jnp.float32) + mixer, inner_norm_gain, inner_norm_bias).astype(jnp.bfloat16)
        gate = jnp.dot(middle, gate_matrix, preferred_element_type=jnp.float32)
        up = jnp.dot(middle, up_matrix, preferred_element_type=jnp.float32)
        hidden = (jax.nn.silu(gate) * up).astype(jnp.bfloat16)
        feed = jnp.zeros((piece_rows, D), jnp.float32)
        for part_index in range(N_TP):
            term = jnp.dot(hidden[:, part_index * share:(part_index + 1) * share], down_matrix[part_index * share:(part_index + 1) * share], preferred_element_type=jnp.float32).astype(jnp.bfloat16)
            feed = feed + lax.optimization_barrier(term).astype(jnp.float32)
        return layer_norm(alpha_mix * middle.astype(jnp.float32) + feed, closing_norm_gain, closing_norm_bias).astype(jnp.bfloat16)
    result = lax.map(finish, (gated.reshape(count, piece_rows, HEADS * HEAD_WIDTH), residual.reshape(count, piece_rows, D)))
    return result.reshape(total, D)
```

```python
import math

import jax
import jax.numpy as jnp
from jax import lax
from jax.experimental import pallas as pl
from jax.experimental.pallas import tpu as pltpu
from jax.sharding import Mesh
from jax.sharding import PartitionSpec as P

D = 2048
SP = ("z", "ya", "yb")
PAIR = ("yb", "tp")
HALF = 384

highest_precision = lax.Precision.HIGHEST
alpha_mix = 2.0**0.25
norm_eps = 1e-05
head_eps = 1e-06


def to_all(x, axes):
    devices = lax.axis_size(axes)
    return lax.all_to_all(jnp.broadcast_to(x[None], (devices, *x.shape)), axes, 0, 0, tiled=True)


def packed_total(arrays, axis):
    vector, at, done = (jnp.concatenate([a.reshape(-1) for a in arrays]), 0, [])
    total = to_all(vector, axis).sum(axis=0)
    for a in arrays:
        done.append(total[at : at + a.size].reshape(a.shape))
        at += a.size
    return tuple(done)


def decay_factors(unscaled_input, lower_bound_gap, extra_decays):
    decay_factor = lower_bound_gap * jax.nn.sigmoid(-unscaled_input.astype(jnp.float32))
    return (jnp.log1p(-decay_factor) + extra_decays, decay_factor)


def local_pass(query, keys, values, log_decay):
    rows = query.shape[0]
    triangle = jnp.tril(jnp.ones((rows, rows), jnp.float32))
    running = jnp.cumsum(log_decay, axis=0)
    total = running[-1]
    decayed_query = query * jnp.exp(running)
    key_inverse = keys * jnp.exp(-running)
    key_stop = keys * jnp.exp(total[None] - running)
    scores = (
        jnp.einsum("tk,sk->ts", decayed_query, key_inverse, precision=highest_precision) * triangle
    )
    inner = jnp.einsum("ts,sv->tv", scores, values, precision=highest_precision)
    state = jnp.einsum("ok,ov->kv", key_stop, values, precision=highest_precision)
    return (inner, decayed_query, total, state)


def scan_kernel(chunks, local_ref, before_ref):
    local = local_ref[...].astype(jnp.float32)
    decay = jnp.exp(local[:, 4:8])
    state = local[:, 0:4]
    ahead = [None] * chunks
    run = jnp.zeros((2, 128), jnp.float32)
    for c in range(chunks):
        ahead[c] = run
        run = decay[c, 0:2] * run + state[c, 0:2]
    run = jnp.zeros((2, 128), jnp.float32)
    for c in reversed(range(chunks)):
        before_ref[c] = jnp.concatenate([ahead[c], run], axis=0)
        run = decay[c, 2:4] * run + state[c, 2:4]


def exchanged_states(forward, backward):
    chunks = lax.axis_size(SP)
    mine = []
    for total, state in (forward, backward):
        mine.append(state.reshape(chunks, 2, 128))
    for total, state in (forward, backward):
        mine.append(jnp.broadcast_to(total.reshape(chunks, 2, 1), (chunks, 2, 128)))
    packed = jnp.concatenate(mine, axis=1).astype(jnp.bfloat16)
    arrived = lax.all_to_all(packed, SP, 0, 0, tiled=True)
    before = pl.pallas_call(
        lambda *refs: scan_kernel(chunks, *refs),
        out_shape=jax.ShapeDtypeStruct((chunks, 4, 128), jnp.float32),
        name="scan",
    )(arrived)
    back = lax.all_to_all(before.astype(jnp.bfloat16), SP, 0, 0, tiled=True).astype(jnp.float32)
    return back[:, 0:2].reshape(128, 128), back[:, 2:4].reshape(128, 128)


def gathered_weights(gate, up, down):
    both = jnp.stack([gate, up, down.T])
    first = both[:, :, :HALF]
    second = jnp.pad(both[:, :, HALF:], ((0, 0), (0, 0), (0, 2 * HALF - both.shape[2])))
    halves = jnp.stack([first, second, first, second])
    arrived = lax.all_to_all(halves, ("ya", "yb"), 0, 0, tiled=True)
    shard = jnp.moveaxis(arrived, 0, 1).reshape(3 * 128, HALF)
    return lax.all_gather(shard, "z", axis=0, tiled=True).reshape(-1, 3, 128, HALF)


def feed_kernel(steps, rows_ref, enter_ref, leave_ref, out_ref, gate_ref, up_ref, hidden_ref):
    phase, step = pl.program_id(0), pl.program_id(1)

    @pl.when(jnp.logical_and(phase == 0, step == 0))
    def _():
        gate_ref[...] = jnp.zeros_like(gate_ref)
        up_ref[...] = jnp.zeros_like(up_ref)

    @pl.when(phase == 0)
    def _():
        x = rows_ref[0]
        gate = jnp.concatenate([enter_ref[0, 0], enter_ref[1, 0]], axis=0)
        up = jnp.concatenate([enter_ref[0, 1], enter_ref[1, 1]], axis=0)
        gate_ref[...] += jnp.dot(x, gate, preferred_element_type=jnp.float32)
        up_ref[...] += jnp.dot(x, up, preferred_element_type=jnp.float32)

    @pl.when(jnp.logical_and(phase == 0, step == steps - 1))
    def _():
        gate = gate_ref[...]
        hidden_ref[...] = (gate * jax.nn.sigmoid(gate) * up_ref[...]).astype(jnp.bfloat16)

    @pl.when(phase == 1)
    def _():
        down = jnp.concatenate([leave_ref[0, 0], leave_ref[1, 0]], axis=0)
        product = lax.dot_general(
            hidden_ref[...],
            down,
            (((1,), (1,)), ((), ())),
            preferred_element_type=jnp.float32,
        )
        out_ref[:, 0] = product.astype(jnp.bfloat16).reshape(out_ref.shape[0], *out_ref.shape[2:])


def feed_forward(rows, weights):
    steps, count, width = rows.shape
    return pl.pallas_call(
        lambda *refs: feed_kernel(steps, *refs),
        grid=(2, steps),
        in_specs=[
            pl.BlockSpec((1, count, width), lambda p, s: (jnp.where(p == 0, s, steps - 1), 0, 0)),
            pl.BlockSpec(
                (2, 2, 128, HALF), lambda p, s: (jnp.where(p == 0, s, steps - 1), 0, 0, 0)
            ),
            pl.BlockSpec((2, 1, 128, HALF), lambda p, s: (jnp.where(p == 0, 0, s), 2, 0, 0)),
        ],
        out_specs=pl.BlockSpec(
            (2, 1, count // 2, width), lambda p, s: (0, jnp.where(p == 0, 0, s), 0, 0)
        ),
        out_shape=jax.ShapeDtypeStruct((2, steps, count // 2, width), jnp.bfloat16),
        scratch_shapes=[
            pltpu.VMEM((count, HALF), jnp.float32),
            pltpu.VMEM((count, HALF), jnp.float32),
            pltpu.VMEM((count, HALF), jnp.bfloat16),
        ],
        compiler_params=pltpu.CompilerParams(dimension_semantics=("arbitrary", "arbitrary")),
        cost_estimate=pl.CostEstimate(
            flops=6 * count * D * HALF, bytes_accessed=6 * D * HALF, transcendentals=count * HALF
        ),
        name="feed_forward",
    )(rows, weights, weights)


def row_norm(before, moments, gain, bias):
    mean = moments[0] / D
    spread = moments[1] / D - mean * mean
    return (before - mean[:, None]) * lax.rsqrt(spread + norm_eps)[:, None] * gain + bias


def shards(
    query_logits,
    value_rows,
    onward_forget_logits,
    reverse_forget_logits,
    output_gate_logits,
    onward_floor_gap,
    reverse_floor_gap,
    extra_log_decay,
    per_head_gain,
    residual,
    output_matrix,
    inner_norm_gain,
    inner_norm_bias,
    gate_matrix,
    up_matrix,
    down_matrix,
    closing_norm_gain,
    closing_norm_bias,
):
    weights = gathered_weights(gate_matrix, up_matrix, down_matrix)
    rows = query_logits.shape[0]
    query = jax.nn.silu(query_logits.astype(jnp.float32))
    values = value_rows.astype(jnp.float32)
    onward_log_decay, onward_keys = decay_factors(
        onward_forget_logits, onward_floor_gap, extra_log_decay
    )
    reverse_log_decay, reverse_keys = decay_factors(
        reverse_forget_logits, reverse_floor_gap, extra_log_decay
    )
    ahead, ahead_query, ahead_total, ahead_state = local_pass(
        query, onward_keys, values, onward_log_decay
    )
    behind, behind_query, behind_total, behind_state = local_pass(
        jnp.flip(query, axis=0),
        jnp.flip(reverse_keys, axis=0),
        jnp.flip(values, axis=0),
        jnp.flip(reverse_log_decay, axis=0),
    )
    incoming, arriving = exchanged_states((ahead_total, ahead_state), (behind_total, behind_state))
    ahead = ahead + jnp.dot(ahead_query, incoming, precision=highest_precision)
    behind = behind + jnp.dot(behind_query, arriving, precision=highest_precision)
    mixed = ahead + jnp.flip(behind, axis=0)
    normed = (
        mixed * lax.rsqrt(jnp.mean(mixed * mixed, axis=1, keepdims=True) + head_eps) * per_head_gain
    )
    gated = (normed * jax.nn.silu(output_gate_logits.astype(jnp.float32))).astype(jnp.bfloat16)
    everyone = to_all(gated, PAIR)
    mixer = jnp.einsum(
        "pthk,hkn->ptn",
        jnp.moveaxis(everyone.reshape(2, -1, rows, 128), 1, 2),
        output_matrix.reshape(-1, 128, output_matrix.shape[1]),
        preferred_element_type=jnp.float32,
    ).reshape(2 * rows, -1)
    pair_residual = to_all(residual, "yb").reshape(2 * rows, -1)
    before_middle = alpha_mix * pair_residual.astype(jnp.float32) + mixer
    moments = packed_total(
        (jnp.sum(before_middle, axis=1), jnp.sum(before_middle * before_middle, axis=1)), "tp"
    )
    middle = row_norm(before_middle, moments, inner_norm_gain, inner_norm_bias).astype(jnp.bfloat16)
    partial_value = feed_forward(to_all(middle, "tp"), weights)
    partial_value = partial_value.reshape(-1, *partial_value.shape[2:])
    feed = lax.all_to_all(partial_value, PAIR, 0, 0, tiled=True).astype(jnp.float32).sum(axis=0)
    own = lax.dynamic_slice_in_dim(middle, lax.axis_index("yb") * rows, rows, 0)
    before_final = alpha_mix * own.astype(jnp.float32) + feed
    closing = packed_total(
        (jnp.sum(before_final, axis=1), jnp.sum(before_final * before_final, axis=1)), "tp"
    )
    return row_norm(before_final, closing, closing_norm_gain, closing_norm_bias).astype(
        jnp.bfloat16
    )


def solution(mesh):
    torus = Mesh(mesh.devices.reshape(16, 2, 2, mesh.shape["tp"]), ("z", "ya", "yb", "tp"))
    in_specs = (
        P(SP, "tp"),
        P(SP, "tp"),
        P(SP, "tp"),
        P(SP, "tp"),
        P(SP, "tp"),
        P("tp"),
        P("tp"),
        P(SP, "tp"),
        P(),
        P(SP, "tp"),
        P(None, "tp"),
        P("tp"),
        P("tp"),
        P(SP, "tp"),
        P(SP, "tp"),
        P("tp", SP),
        P("tp"),
        P("tp"),
    )
    out_specs = P(SP, "tp")
    return jax.shard_map(
        shards, mesh=torus, in_specs=in_specs, out_specs=out_specs, check_vma=False
    )
```

```python
import math

import jax
import jax.numpy as jnp
from jax import lax
from jax.experimental import pallas as pl
from jax.experimental.pallas import tpu as pltpu
from jax.sharding import Mesh
from jax.sharding import PartitionSpec as P

D = 2048
SP = ("z", "ya", "yb")
TP = ("x", "c")
PAIR = ("yb", "x", "c")
HALF = 384

highest_precision = lax.Precision.HIGHEST
alpha_mix = 2.0**0.25
norm_eps = 1e-05
head_eps = 1e-06


def to_all(x, axes):
    devices = lax.axis_size(axes)
    return lax.all_to_all(jnp.broadcast_to(x[None], (devices, *x.shape)), axes, 0, 0, tiled=True)


def packed_total(arrays, axis):
    vector, at, done = (jnp.concatenate([a.reshape(-1) for a in arrays]), 0, [])
    total = to_all(vector, axis).sum(axis=0)
    for a in arrays:
        done.append(total[at : at + a.size].reshape(a.shape))
        at += a.size
    return tuple(done)


def local_kernel(
    query_ref,
    value_ref,
    onward_ref,
    reverse_ref,
    onward_gap_ref,
    reverse_gap_ref,
    extra_ref,
    inner_ref,
    queries_ref,
    states_ref,
    totals_ref,
):
    def dot(a, b, dims=((1,), (0,))):
        return lax.dot_general(
            a, b, (dims, ((), ())), precision=highest_precision, preferred_element_type=jnp.float32
        )

    rows = query_ref.shape[0]
    logits = query_ref[...].astype(jnp.float32)
    query = logits / (1.0 + jnp.exp(-logits))
    values = value_ref[...].astype(jnp.float32)
    at = lax.broadcasted_iota(jnp.int32, (rows, rows), 0)
    source = lax.broadcasted_iota(jnp.int32, (rows, rows), 1)
    inner = jnp.zeros_like(query)
    for side, (forget_ref, gap_ref, seen, last) in enumerate(
        ((onward_ref, onward_gap_ref, at >= source, rows - 1), (reverse_ref, reverse_gap_ref, at <= source, 0))
    ):
        seen = seen.astype(jnp.float32)
        keys = gap_ref[...] / (1.0 + jnp.exp(forget_ref[...].astype(jnp.float32)))
        running = dot(seen, jnp.log1p(-keys) + extra_ref[...])
        total = running[last : last + 1]
        decayed_query = query * jnp.exp(running)
        scores = dot(decayed_query, keys * jnp.exp(-running), ((1,), (1,))) * seen
        inner = inner + dot(scores, values)
        queries_ref[:, 128 * side : 128 * side + 128] = decayed_query
        states_ref[side] = dot(keys * jnp.exp(total - running), values, ((0,), (0,)))
        totals_ref[side : side + 1] = total
    inner_ref[...] = inner


def local_pass(query, values, onward, reverse, onward_gap, reverse_gap, extra):
    rows, width = query.shape
    shapes = ((rows, width), (rows, 2 * width), (2, width, width), (2, width))
    return pl.pallas_call(
        local_kernel,
        out_shape=[jax.ShapeDtypeStruct(s, jnp.float32) for s in shapes],
        name="local",
    )(query, values, onward, reverse, onward_gap[None], reverse_gap[None], extra)


def scan_kernel(chunks, local_ref, before_ref):
    local = local_ref[...].astype(jnp.float32)
    decay = jnp.exp(local[:, 4:8])
    state = local[:, 0:4]
    ahead = [None] * chunks
    run = jnp.zeros((2, 128), jnp.float32)
    for c in range(chunks):
        ahead[c] = run
        run = decay[c, 0:2] * run + state[c, 0:2]
    run = jnp.zeros((2, 128), jnp.float32)
    for c in reversed(range(chunks)):
        before_ref[c] = jnp.concatenate([ahead[c], run], axis=0).astype(jnp.bfloat16)
        run = decay[c, 2:4] * run + state[c, 2:4]


def exchanged_states(states, totals):
    chunks = lax.axis_size(SP)
    decays = jnp.broadcast_to(totals.reshape(4, chunks, 1), (4, chunks, 128))
    packed = jnp.concatenate([states.reshape(4, chunks, 128), decays])
    packed = jnp.moveaxis(packed.astype(jnp.bfloat16), 1, 0)
    arrived = lax.all_to_all(packed, SP, 0, 0, tiled=True)
    before = pl.pallas_call(
        lambda *refs: scan_kernel(chunks, *refs),
        out_shape=jax.ShapeDtypeStruct((chunks, 4, 128), jnp.bfloat16),
        name="scan",
    )(arrived)
    back = lax.all_to_all(before, SP, 0, 0, tiled=True).astype(jnp.float32)
    return jnp.moveaxis(back, 1, 0).reshape(4 * chunks, 128)


def gathered_weights(gate, up, down):
    both = jnp.stack([gate, up, down.T])
    first = both[:, :, :HALF]
    second = jnp.pad(both[:, :, HALF:], ((0, 0), (0, 0), (0, 2 * HALF - both.shape[2])))
    halves = jnp.stack([first, second, first, second])
    arrived = lax.all_to_all(halves, ("ya", "yb"), 0, 0, tiled=True)
    shard = jnp.moveaxis(arrived, 0, 1).reshape(3 * 128, HALF)
    return lax.all_gather(shard, "z", axis=0, tiled=True).reshape(-1, 3, 128, HALF)


def exact_terms(x):
    terms = []
    for _ in range(3):
        term = lax.reduce_precision(x, 8, 7)
        terms.append(term.astype(jnp.bfloat16))
        x = x - term
    return terms


def whole_columns(output_matrix, residual, gain, bias):
    rows = residual.shape[0]
    other = lax.ppermute(residual, "yb", ((0, 1), (1, 0)))
    first = lax.axis_index("yb") == 0
    vectors = jnp.stack(exact_terms(gain) + exact_terms(bias))
    block = jnp.concatenate(
        [
            output_matrix,
            jnp.where(first, residual, other),
            jnp.where(first, other, residual),
            jnp.pad(vectors, ((0, 10), (0, 0))),
        ]
    )
    both = jnp.stack([block, lax.ppermute(block, "c", ((0, 1), (1, 0)))])
    count = lax.axis_size("x")
    return [both] + [
        lax.ppermute(both, "x", [(i, (i + k) % count) for i in range(count)])
        for k in range(1, count)
    ]


def middle_kernel(place_ref, gated_ref, *refs):
    block_refs, (out_ref, whole_ref, before_ref) = refs[:4], refs[4:]
    heads, rows = 8, gated_ref.shape[2]
    count = 2 * rows
    for core in range(2):
        for pair in range(2):
            for x in range(4):
                head = 2 * x + core
                whole_ref[pair * rows : (pair + 1) * rows, 128 * head : 128 * head + 128] = (
                    gated_ref[core, 4 * pair + x]
                )
    whole = whole_ref[...]
    inner = whole.shape[1]
    total = jnp.zeros((count, 1), jnp.float32)
    for b in range(heads):
        block_ref = block_refs[b // 2]
        mixer = jnp.dot(whole, block_ref[b % 2, :inner], preferred_element_type=jnp.float32)
        residual = block_ref[b % 2, inner : inner + count].astype(jnp.float32)
        before = alpha_mix * residual + mixer
        before_ref[b] = before
        total = total + jnp.sum(before, axis=1, keepdims=True)
    mean = total / D
    spread = jnp.zeros((count, 1), jnp.float32)
    for b in range(heads):
        centre = before_ref[b] - mean
        spread = spread + jnp.sum(centre * centre, axis=1, keepdims=True)
    scale = lax.rsqrt(spread / D + norm_eps)
    for b in range(heads):
        vectors = block_refs[b // 2][b % 2, inner + count : inner + count + 16].astype(jnp.float32)
        gain = vectors[0:1] + vectors[1:2] + vectors[2:3]
        bias = vectors[3:4] + vectors[4:5] + vectors[5:6]
        normed = (before_ref[b] - mean) * scale * gain + bias
        out_ref[place_ref[b]] = normed.astype(jnp.bfloat16)


def middle_rows(gated, blocks):
    rows, width = gated.shape[2], blocks[0].shape[2]
    x, core = lax.axis_index("x"), lax.axis_index("c")
    place = jnp.stack([2 * ((x - b // 2 + 4) % 4) + (core + b) % 2 for b in range(8)])
    vmem = pl.BlockSpec(memory_space=pltpu.VMEM)
    return pl.pallas_call(
        middle_kernel,
        in_specs=[pl.BlockSpec(memory_space=pltpu.SMEM)] + [vmem] * 5,
        out_specs=vmem,
        out_shape=jax.ShapeDtypeStruct((8, 2 * rows, width), jnp.bfloat16),
        scratch_shapes=[
            pltpu.VMEM((2 * rows, 8 * 128), jnp.bfloat16),
            pltpu.VMEM((8, 2 * rows, width), jnp.float32),
        ],
        name="middle",
    )(place.astype(jnp.int32), gated, *blocks)


def feed_kernel(steps, rows_ref, enter_ref, leave_ref, out_ref, gate_ref, up_ref, hidden_ref):
    phase, step = pl.program_id(0), pl.program_id(1)

    @pl.when(jnp.logical_and(phase == 0, step == 0))
    def _():
        gate_ref[...] = jnp.zeros_like(gate_ref)
        up_ref[...] = jnp.zeros_like(up_ref)

    @pl.when(phase == 0)
    def _():
        for to_ref, kind in ((gate_ref, 0), (up_ref, 1)):
            product = 0.0
            for b in range(rows_ref.shape[0]):
                wide = jnp.concatenate([enter_ref[2 * b, kind], enter_ref[2 * b + 1, kind]], axis=0)
                product += jnp.dot(rows_ref[b], wide, preferred_element_type=jnp.float32)
            to_ref[...] += product

    @pl.when(jnp.logical_and(phase == 0, step == steps - 1))
    def _():
        gate = gate_ref[...]
        hidden_ref[...] = (gate / (1.0 + jnp.exp(-gate)) * up_ref[...]).astype(jnp.bfloat16)

    @pl.when(phase == 1)
    def _():
        for b in range(out_ref.shape[1]):
            down = jnp.concatenate([leave_ref[2 * b, 0], leave_ref[2 * b + 1, 0]], axis=0)
            product = lax.dot_general(
                hidden_ref[...],
                down,
                (((1,), (1,)), ((), ())),
                preferred_element_type=jnp.float32,
            ).astype(jnp.bfloat16)
            for pair in range(2):
                rows = out_ref.shape[2]
                out_ref[pair, b] = product[pair * rows : (pair + 1) * rows]


def feed_forward(rows, weights):
    blocks, count, width = rows.shape
    each = 2
    steps = blocks // each
    return pl.pallas_call(
        lambda *refs: feed_kernel(steps, *refs),
        grid=(2, steps),
        in_specs=[
            pl.BlockSpec((each, count, width), lambda p, s: (jnp.where(p == 0, s, steps - 1), 0, 0)),
            pl.BlockSpec(
                (2 * each, 2, 128, HALF), lambda p, s: (jnp.where(p == 0, s, steps - 1), 0, 0, 0)
            ),
            pl.BlockSpec((2 * each, 1, 128, HALF), lambda p, s: (jnp.where(p == 0, 0, s), 2, 0, 0)),
        ],
        out_specs=pl.BlockSpec(
            (2, each, count // 2, width), lambda p, s: (0, jnp.where(p == 0, 0, s), 0, 0)
        ),
        out_shape=jax.ShapeDtypeStruct((2, blocks, count // 2, width), jnp.bfloat16),
        scratch_shapes=[
            pltpu.VMEM((count, HALF), jnp.float32),
            pltpu.VMEM((count, HALF), jnp.float32),
            pltpu.VMEM((count, HALF), jnp.bfloat16),
        ],
        compiler_params=pltpu.CompilerParams(dimension_semantics=("arbitrary", "arbitrary")),
        cost_estimate=pl.CostEstimate(
            flops=6 * count * D * HALF, bytes_accessed=6 * D * HALF, transcendentals=count * HALF
        ),
        name="feed_forward",
    )(rows, weights, weights)


def row_norm(before, moments, gain, bias):
    mean = moments[0] / D
    spread = moments[1] / D - mean * mean
    return (before - mean[:, None]) * lax.rsqrt(spread + norm_eps)[:, None] * gain + bias


def shards(
    query_logits,
    value_rows,
    onward_forget_logits,
    reverse_forget_logits,
    output_gate_logits,
    onward_floor_gap,
    reverse_floor_gap,
    extra_log_decay,
    per_head_gain,
    residual,
    output_matrix,
    inner_norm_gain,
    inner_norm_bias,
    gate_matrix,
    up_matrix,
    down_matrix,
    closing_norm_gain,
    closing_norm_bias,
):
    weights = gathered_weights(gate_matrix, up_matrix, down_matrix)
    blocks = whole_columns(output_matrix, residual, inner_norm_gain, inner_norm_bias)
    rows = query_logits.shape[0]
    inner, queries, states, totals = local_pass(
        query_logits,
        value_rows,
        onward_forget_logits,
        reverse_forget_logits,
        onward_floor_gap,
        reverse_floor_gap,
        extra_log_decay,
    )
    mixed = inner + jnp.dot(queries, exchanged_states(states, totals), precision=highest_precision)
    normed = (
        mixed * lax.rsqrt(jnp.mean(mixed * mixed, axis=1, keepdims=True) + head_eps) * per_head_gain
    )
    gated = (normed * jax.nn.silu(output_gate_logits.astype(jnp.float32))).astype(jnp.bfloat16)
    everyone = lax.all_gather(to_all(gated, ("yb", "x")), "c")
    middle = middle_rows(everyone, blocks)
    partial_value = feed_forward(middle, weights)
    partial_value = partial_value.reshape(-1, *partial_value.shape[2:])
    feed = lax.all_to_all(partial_value, PAIR, 0, 0, tiled=True).astype(jnp.float32).sum(axis=0)
    own = lax.dynamic_slice(
        middle,
        (lax.axis_index(TP), lax.axis_index("yb") * rows, 0),
        (1, rows, middle.shape[2]),
    )[0]
    before_final = alpha_mix * own.astype(jnp.float32) + feed
    closing = packed_total(
        (jnp.sum(before_final, axis=1), jnp.sum(before_final * before_final, axis=1)), TP
    )
    return row_norm(before_final, closing, closing_norm_gain, closing_norm_bias).astype(
        jnp.bfloat16
    )


def solution(mesh):
    torus = Mesh(mesh.devices.reshape(16, 2, 2, 4, 2), ("z", "ya", "yb", "x", "c"))
    in_specs = (
        P(SP, TP),
        P(SP, TP),
        P(SP, TP),
        P(SP, TP),
        P(SP, TP),
        P(TP),
        P(TP),
        P(SP, TP),
        P(),
        P(SP, TP),
        P(None, TP),
        P(TP),
        P(TP),
        P(SP, TP),
        P(SP, TP),
        P(TP, SP),
        P(TP),
        P(TP),
    )
    out_specs = P(SP, TP)
    return jax.shard_map(
        shards, mesh=torus, in_specs=in_specs, out_specs=out_specs, check_vma=False
    )
```

```python
import jax
import jax.numpy as jnp
from jax import lax
from jax.experimental import pallas as pl
from jax.experimental.pallas import tpu as pltpu
from jax.sharding import Mesh
from jax.sharding import PartitionSpec as P


D = 2048
SP = ("z", "ya", "yb")
TP = ("x", "c")
HALF = 384

highest_precision = lax.Precision.HIGHEST
alpha_mix = 2.0**0.25
norm_eps = 1e-05
head_eps = 1e-06


def exact_dot(a, b, dims=((1,), (0,))):
    return lax.dot_general(
        a, b, (dims, ((), ())), precision=highest_precision, preferred_element_type=jnp.float32
    )


def local_kernel(
    query_ref,
    value_ref,
    onward_ref,
    reverse_ref,
    onward_gap_ref,
    reverse_gap_ref,
    extra_ref,
    inner_ref,
    queries_ref,
    packed_ref,
    rows_ref,
):
    rows, width = query_ref.shape
    half = width // 2
    logits = query_ref[...].astype(jnp.float32)
    query = logits / (1.0 + jnp.exp(-logits))
    values = value_ref[...].astype(jnp.float32)
    extra = extra_ref[...]
    at = lax.broadcasted_iota(jnp.int32, (rows, rows), 0)
    source = lax.broadcasted_iota(jnp.int32, (rows, rows), 1)
    ones = jnp.ones((rows, width), jnp.float32)
    inner = jnp.zeros_like(query)
    for side, (forget_ref, gap_ref, seen, last) in enumerate(
        (
            (onward_ref, onward_gap_ref, at >= source, rows - 1),
            (reverse_ref, reverse_gap_ref, at <= source, 0),
        )
    ):
        seen = seen.astype(jnp.float32)
        keys = gap_ref[...] / (1.0 + jnp.exp(forget_ref[...].astype(jnp.float32)))
        log_decay = jnp.log1p(-keys)
        running = exact_dot(seen, log_decay) + exact_dot(seen * extra, ones)
        total = running[last : last + 1]
        decayed_query = query * jnp.exp(running)
        scores = exact_dot(decayed_query, keys * jnp.exp(-running), ((1,), (1,))) * seen
        inner = inner + exact_dot(scores, values)
        queries_ref[:, width * side : width * (side + 1)] = decayed_query
        state = exact_dot(keys * jnp.exp(total - running), values, ((0,), (0,)))
        decay = exact_dot(log_decay, ones, ((0,), (0,))) + jnp.sum(extra)
        for part in range(2):
            rows_ref[:, 2 * side + part, :] = state[part * half : (part + 1) * half]
            rows_ref[:, 4 + 2 * side + part, :] = decay[part * half : (part + 1) * half]
    packed_ref[...] = rows_ref[...].astype(jnp.bfloat16)
    inner_ref[...] = inner


def local_pass(query, values, onward, reverse, onward_gap, reverse_gap, extra):
    rows, width = query.shape
    half = width // 2
    return pl.pallas_call(
        local_kernel,
        out_shape=[
            jax.ShapeDtypeStruct((rows, width), jnp.float32),
            jax.ShapeDtypeStruct((rows, 2 * width), jnp.float32),
            jax.ShapeDtypeStruct((half, 8, width), jnp.bfloat16),
        ],
        scratch_shapes=[pltpu.VMEM((half, 8, width), jnp.float32)],
        name="local",
    )(query, values, onward, reverse, onward_gap[None], reverse_gap[None], extra.reshape(1, rows))


def gated_kernel(back_ref, inner_ref, queries_ref, gain_ref, gate_ref, out_ref, states_ref):
    states_ref[...] = back_ref[...].astype(jnp.float32)
    width = inner_ref.shape[1]
    mixed = inner_ref[...]
    for side in range(2):
        state = jnp.concatenate([states_ref[:, 2 * side, :], states_ref[:, 2 * side + 1, :]], axis=0)
        mixed = mixed + exact_dot(queries_ref[:, width * side : width * (side + 1)], state)
    mean = jnp.mean(mixed * mixed, axis=1, keepdims=True)
    normed = mixed * lax.rsqrt(mean + head_eps) * gain_ref[...]
    gate = gate_ref[...].astype(jnp.float32)
    gated = (normed * (gate / (1.0 + jnp.exp(-gate)))).astype(jnp.bfloat16)
    for peer in range(out_ref.shape[0]):
        out_ref[peer] = gated


def gated_rows(back, inner, queries, gain, gate, peers):
    return pl.pallas_call(
        gated_kernel,
        out_shape=jax.ShapeDtypeStruct((peers, *inner.shape), jnp.bfloat16),
        scratch_shapes=[pltpu.VMEM(back.shape, jnp.float32)],
        name="gated",
    )(back, inner, queries, gain[None], gate)


def scan_kernel(chunks, local_ref, before_ref):
    local = local_ref[...].astype(jnp.float32)
    decay = jnp.exp(local[:, 4:8])
    state = local[:, 0:4]
    ahead = [None] * chunks
    run = jnp.zeros((2, 128), jnp.float32)
    for c in range(chunks):
        ahead[c] = run
        run = decay[c, 0:2] * run + state[c, 0:2]
    run = jnp.zeros((2, 128), jnp.float32)
    for c in reversed(range(chunks)):
        before_ref[c] = jnp.concatenate([ahead[c], run], axis=0).astype(jnp.bfloat16)
        run = decay[c, 2:4] * run + state[c, 2:4]


def scanned(arrived):
    chunks = arrived.shape[0]
    return pl.pallas_call(
        lambda *refs: scan_kernel(chunks, *refs),
        out_shape=jax.ShapeDtypeStruct((chunks, 4, 128), jnp.bfloat16),
        name="scan",
    )(arrived)


def gathered_weights(gate, up, down):
    both = jnp.stack([gate, up, down.T])
    first = both[:, :, :HALF]
    second = jnp.pad(both[:, :, HALF:], ((0, 0), (0, 0), (0, 2 * HALF - both.shape[2])))
    halves = jnp.stack([first, second, first, second])
    arrived = lax.all_to_all(halves, ("ya", "yb"), 0, 0, tiled=True)
    shard = jnp.moveaxis(arrived, 0, 1).reshape(3 * 128, HALF)
    return lax.all_gather(shard, "z", axis=0, tiled=True).reshape(-1, 3, 128, HALF)


def exact_terms(x):
    terms = []
    for _ in range(3):
        term = lax.reduce_precision(x, 8, 7)
        terms.append(term.astype(jnp.bfloat16))
        x = x - term
    return terms


SWAP = ((0, 1), (1, 0))


def spread_over_x(output_matrix, residual, gain, bias):
    other = lax.ppermute(residual, "yb", SWAP)
    first = lax.axis_index("yb") == 0
    vectors = jnp.stack(exact_terms(gain) + exact_terms(bias))
    block = jnp.concatenate(
        [
            output_matrix,
            jnp.where(first, residual, other),
            jnp.where(first, other, residual),
            jnp.pad(vectors, ((0, 10), (0, 0))),
        ]
    )
    count = lax.axis_size("x")
    return [block] + [
        lax.ppermute(block, "x", [(i, (i + k) % count) for i in range(count)])
        for k in range(1, count)
    ]


def middle_kernel(place_ref, gated_ref, *refs):
    block_refs, (out_ref, whole_ref, before_ref) = refs[:8], refs[8:]
    heads, rows = 8, gated_ref.shape[2]
    count = 2 * rows
    for core in range(2):
        for pair in range(2):
            for x in range(4):
                head = 2 * x + core
                whole_ref[pair * rows : (pair + 1) * rows, 128 * head : 128 * head + 128] = (
                    gated_ref[core, 4 * pair + x]
                )
    whole = whole_ref[...]
    inner = whole.shape[1]
    total = jnp.zeros((count, 1), jnp.float32)
    for b in range(heads):
        mixer = jnp.dot(whole, block_refs[b][:inner], preferred_element_type=jnp.float32)
        residual = block_refs[b][inner : inner + count].astype(jnp.float32)
        before = alpha_mix * residual + mixer
        before_ref[b] = before
        total = total + jnp.sum(before, axis=1, keepdims=True)
    mean = total / D
    spread = jnp.zeros((count, 1), jnp.float32)
    for b in range(heads):
        centre = before_ref[b] - mean
        spread = spread + jnp.sum(centre * centre, axis=1, keepdims=True)
    scale = lax.rsqrt(spread / D + norm_eps)
    for b in range(heads):
        vectors = block_refs[b][inner + count : inner + count + 16].astype(jnp.float32)
        gain = vectors[0:1] + vectors[1:2] + vectors[2:3]
        bias = vectors[3:4] + vectors[4:5] + vectors[5:6]
        normed = (before_ref[b] - mean) * scale * gain + bias
        out_ref[place_ref[b]] = normed.astype(jnp.bfloat16)


def middle_rows(gated, blocks):
    rows, width = gated.shape[2], blocks[0].shape[1]
    x, core = lax.axis_index("x"), lax.axis_index("c")
    place = jnp.stack([2 * ((x - b // 2 + 4) % 4) + (core + b) % 2 for b in range(8)])
    vmem = pl.BlockSpec(memory_space=pltpu.VMEM)
    return pl.pallas_call(
        middle_kernel,
        in_specs=[pl.BlockSpec(memory_space=pltpu.SMEM)] + [vmem] * 9,
        out_specs=vmem,
        out_shape=jax.ShapeDtypeStruct((8, 2 * rows, width), jnp.bfloat16),
        scratch_shapes=[
            pltpu.VMEM((2 * rows, 8 * 128), jnp.bfloat16),
            pltpu.VMEM((8, 2 * rows, width), jnp.float32),
        ],
        name="middle",
    )(place.astype(jnp.int32), gated, *blocks)


def feed_kernel(
    steps, core_ref, rows_ref, enter_ref, leave_ref, keep_ref, send_ref, gate_ref, up_ref, hidden_ref
):
    phase, step = pl.program_id(0), pl.program_id(1)

    @pl.when(jnp.logical_and(phase == 0, step == 0))
    def _():
        gate_ref[...] = jnp.zeros_like(gate_ref)
        up_ref[...] = jnp.zeros_like(up_ref)

    @pl.when(phase == 0)
    def _():
        for to_ref, kind in ((gate_ref, 0), (up_ref, 1)):
            product = 0.0
            for b in range(rows_ref.shape[0]):
                wide = jnp.concatenate([enter_ref[2 * b, kind], enter_ref[2 * b + 1, kind]], axis=0)
                product += jnp.dot(rows_ref[b], wide, preferred_element_type=jnp.float32)
            to_ref[...] += product

    @pl.when(jnp.logical_and(phase == 0, step == steps - 1))
    def _():
        gate = gate_ref[...]
        hidden_ref[...] = (gate / (1.0 + jnp.exp(-gate)) * up_ref[...]).astype(jnp.bfloat16)

    @pl.when(phase == 1)
    def _():
        core = core_ref[0]
        for to_ref, b in ((keep_ref, core), (send_ref, 1 - core)):
            down = jnp.concatenate([leave_ref[2 * b, 0], leave_ref[2 * b + 1, 0]], axis=0)
            product = lax.dot_general(
                hidden_ref[...],
                down,
                (((1,), (1,)), ((), ())),
                preferred_element_type=jnp.float32,
            ).astype(jnp.bfloat16)
            for pair in range(2):
                rows = to_ref.shape[2]
                to_ref[pair, 0] = product[pair * rows : (pair + 1) * rows]


def feed_forward(rows, weights):
    blocks, count, width = rows.shape
    each = 2
    steps = blocks // each
    out = jax.ShapeDtypeStruct((2, steps, count // 2, width), jnp.bfloat16)
    out_spec = pl.BlockSpec(
        (2, 1, count // 2, width), lambda p, s, c: (0, jnp.where(p == 0, 0, s), 0, 0)
    )
    return pl.pallas_call(
        lambda *refs: feed_kernel(steps, *refs),
        grid_spec=pltpu.PrefetchScalarGridSpec(
            num_scalar_prefetch=1,
            grid=(2, steps),
            in_specs=[
                pl.BlockSpec(
                    (each, count, width), lambda p, s, c: (jnp.where(p == 0, s, steps - 1), 0, 0)
                ),
                pl.BlockSpec(
                    (2 * each, 2, 128, HALF),
                    lambda p, s, c: (jnp.where(p == 0, s, steps - 1), 0, 0, 0),
                ),
                pl.BlockSpec(
                    (2 * each, 1, 128, HALF), lambda p, s, c: (jnp.where(p == 0, 0, s), 2, 0, 0)
                ),
            ],
            out_specs=[out_spec, out_spec],
            scratch_shapes=[
                pltpu.VMEM((count, HALF), jnp.float32),
                pltpu.VMEM((count, HALF), jnp.float32),
                pltpu.VMEM((count, HALF), jnp.bfloat16),
            ],
        ),
        out_shape=[out, out],
        compiler_params=pltpu.CompilerParams(dimension_semantics=("arbitrary", "arbitrary")),
        cost_estimate=pl.CostEstimate(
            flops=6 * count * D * HALF, bytes_accessed=6 * D * HALF, transcendentals=count * HALF
        ),
        name="feed_forward",
    )(lax.axis_index("c").astype(jnp.int32)[None], rows, weights, weights)


def total_kernel(arrived_ref, own_ref, before_ref, moments_ref):
    feed = arrived_ref[0].astype(jnp.float32)
    for peer in range(1, arrived_ref.shape[0]):
        feed = feed + arrived_ref[peer].astype(jnp.float32)
    before = alpha_mix * own_ref[...].astype(jnp.float32) + feed
    before_ref[...] = before
    ones = jnp.ones((8, before.shape[1]), jnp.float32)
    sums = exact_dot(ones, before, ((1,), (1,)))
    squares = exact_dot(ones, before * before, ((1,), (1,)))
    moments = jnp.concatenate([sums[0:4], squares[0:4]], axis=0)
    for peer in range(moments_ref.shape[0]):
        moments_ref[peer] = moments


def closing_kernel(moments_ref, before_ref, gain_ref, bias_ref, out_ref):
    moments = moments_ref[0]
    for peer in range(1, moments_ref.shape[0]):
        moments = moments + moments_ref[peer]
    mean = moments[0:1] / D
    spread = moments[4:5] / D - mean * mean
    scale = lax.rsqrt(spread + norm_eps)
    rows, _ = before_ref.shape
    at = lax.broadcasted_iota(jnp.int32, (rows, rows), 0)
    diagonal = (at == lax.broadcasted_iota(jnp.int32, (rows, rows), 1)).astype(jnp.float32)
    column = jnp.sum(diagonal * mean, axis=1, keepdims=True)
    factor = jnp.sum(diagonal * scale, axis=1, keepdims=True)
    out_ref[...] = ((before_ref[...] - column) * factor * gain_ref[...] + bias_ref[...]).astype(
        jnp.bfloat16
    )


def layer(
    query_logits,
    value_rows,
    onward_forget_logits,
    reverse_forget_logits,
    output_gate_logits,
    onward_floor_gap,
    reverse_floor_gap,
    extra_log_decay,
    per_head_gain,
    residual,
    output_matrix,
    inner_norm_gain,
    inner_norm_bias,
    gate_matrix,
    up_matrix,
    down_matrix,
    closing_norm_gain,
    closing_norm_bias,
):
    weights = gathered_weights(gate_matrix, up_matrix, down_matrix)
    rows = query_logits.shape[0]
    inner, queries, packed = local_pass(
        query_logits,
        value_rows,
        onward_forget_logits,
        reverse_forget_logits,
        onward_floor_gap,
        reverse_floor_gap,
        extra_log_decay,
    )
    packed, output_matrix, residual = lax.optimization_barrier((packed, output_matrix, residual))
    arrived = lax.all_to_all(packed, SP, 0, 0, tiled=True)
    blocks = spread_over_x(output_matrix, residual, inner_norm_gain, inner_norm_bias)
    before, *blocks = lax.optimization_barrier((scanned(arrived), *blocks))
    back = lax.all_to_all(before, SP, 0, 0, tiled=True)
    both = []
    for block in blocks:
        both += [block, lax.ppermute(block, "c", SWAP)]
    gated = gated_rows(back, inner, queries, per_head_gain, output_gate_logits, 8)
    everyone = lax.all_gather(lax.all_to_all(gated, ("yb", "x"), 0, 0, tiled=True), "c")
    middle = middle_rows(everyone, both)
    keep, send = feed_forward(middle, weights)
    joined = keep.astype(jnp.float32) + lax.ppermute(send, "c", SWAP).astype(jnp.float32)
    joined = joined.astype(jnp.bfloat16).reshape(-1, *keep.shape[2:])
    shares = lax.all_to_all(joined, ("yb", "x"), 0, 0, tiled=True)
    own = lax.dynamic_slice(
        middle,
        (lax.axis_index(TP), lax.axis_index("yb") * rows, 0),
        (1, rows, middle.shape[2]),
    )[0]
    before_final, moments = pl.pallas_call(
        total_kernel,
        out_shape=[
            jax.ShapeDtypeStruct(own.shape, jnp.float32),
            jax.ShapeDtypeStruct((8, 8, rows), jnp.float32),
        ],
        name="total",
    )(shares, own)
    return pl.pallas_call(
        closing_kernel,
        out_shape=jax.ShapeDtypeStruct(own.shape, jnp.bfloat16),
        name="closing",
    )(
        lax.all_to_all(moments, TP, 0, 0, tiled=True),
        before_final,
        closing_norm_gain[None],
        closing_norm_bias[None],
    )


def solution(mesh):
    torus = Mesh(mesh.devices.reshape(16, 2, 2, 4, 2), ("z", "ya", "yb", "x", "c"))
    in_specs = (
        P(SP, TP),
        P(SP, TP),
        P(SP, TP),
        P(SP, TP),
        P(SP, TP),
        P(TP),
        P(TP),
        P(SP, TP),
        P(),
        P(SP, TP),
        P(None, TP),
        P(TP),
        P(TP),
        P(SP, TP),
        P(SP, TP),
        P(TP, SP),
        P(TP),
        P(TP),
    )
    out_specs = P(SP, TP)
    return jax.shard_map(layer, mesh=torus, in_specs=in_specs, out_specs=out_specs, check_vma=False)
```

```python
import jax
import jax.numpy as jnp
from jax import lax
from jax.experimental import pallas as pl
from jax.experimental.pallas import tpu as pltpu
from jax.sharding import Mesh
from jax.sharding import PartitionSpec as P


D = 2048
SP = ("z", "ya", "yb")
TP = ("x", "c")
HALF = 384

highest_precision = lax.Precision.HIGHEST
alpha_mix = 2.0**0.25
norm_eps = 1e-05
head_eps = 1e-06


def exact_dot(a, b, dims=((1,), (0,))):
    return lax.dot_general(
        a, b, (dims, ((), ())), precision=highest_precision, preferred_element_type=jnp.float32
    )


def local_kernel(
    query_ref,
    value_ref,
    onward_ref,
    reverse_ref,
    onward_gap_ref,
    reverse_gap_ref,
    extra_ref,
    inner_ref,
    queries_ref,
    packed_ref,
    rows_ref,
):
    rows, width = query_ref.shape
    half = width // 2
    logits = query_ref[...].astype(jnp.float32)
    query = logits / (1.0 + jnp.exp(-logits))
    values = value_ref[...].astype(jnp.float32)
    extra = extra_ref[...]
    at = lax.broadcasted_iota(jnp.int32, (rows, rows), 0)
    source = lax.broadcasted_iota(jnp.int32, (rows, rows), 1)
    ones = jnp.ones((rows, width), jnp.float32)
    inner = jnp.zeros_like(query)
    for side, (forget_ref, gap_ref, seen, last) in enumerate(
        (
            (onward_ref, onward_gap_ref, at >= source, rows - 1),
            (reverse_ref, reverse_gap_ref, at <= source, 0),
        )
    ):
        seen = seen.astype(jnp.float32)
        keys = gap_ref[...] / (1.0 + jnp.exp(forget_ref[...].astype(jnp.float32)))
        log_decay = jnp.log1p(-keys)
        running = exact_dot(seen, log_decay) + exact_dot(seen * extra, ones)
        total = running[last : last + 1]
        decayed_query = query * jnp.exp(running)
        scores = exact_dot(decayed_query, keys * jnp.exp(-running), ((1,), (1,))) * seen
        inner = inner + exact_dot(scores, values)
        queries_ref[:, width * side : width * (side + 1)] = decayed_query
        state = exact_dot(keys * jnp.exp(total - running), values, ((0,), (0,)))
        decay = exact_dot(log_decay, ones, ((0,), (0,))) + jnp.sum(extra)
        for part in range(2):
            rows_ref[:, 2 * side + part, :] = state[part * half : (part + 1) * half]
            rows_ref[:, 4 + 2 * side + part, :] = decay[part * half : (part + 1) * half]
    packed_ref[...] = rows_ref[...].astype(jnp.bfloat16)
    inner_ref[...] = inner


def local_pass(query, values, onward, reverse, onward_gap, reverse_gap, extra):
    rows, width = query.shape
    half = width // 2
    return pl.pallas_call(
        local_kernel,
        out_shape=[
            jax.ShapeDtypeStruct((rows, width), jnp.float32),
            jax.ShapeDtypeStruct((rows, 2 * width), jnp.float32),
            jax.ShapeDtypeStruct((half, 8, width), jnp.bfloat16),
        ],
        scratch_shapes=[pltpu.VMEM((half, 8, width), jnp.float32)],
        name="local",
    )(query, values, onward, reverse, onward_gap[None], reverse_gap[None], extra.reshape(1, rows))


def gated_kernel(back_ref, inner_ref, queries_ref, gain_ref, gate_ref, out_ref, states_ref):
    states_ref[...] = back_ref[...].astype(jnp.float32)
    width = inner_ref.shape[1]
    mixed = inner_ref[...]
    for side in range(2):
        state = jnp.concatenate([states_ref[:, 2 * side, :], states_ref[:, 2 * side + 1, :]], axis=0)
        mixed = mixed + exact_dot(queries_ref[:, width * side : width * (side + 1)], state)
    mean = jnp.mean(mixed * mixed, axis=1, keepdims=True)
    normed = mixed * lax.rsqrt(mean + head_eps) * gain_ref[...]
    gate = gate_ref[...].astype(jnp.float32)
    gated = (normed * (gate / (1.0 + jnp.exp(-gate)))).astype(jnp.bfloat16)
    for peer in range(out_ref.shape[0]):
        out_ref[peer] = gated


def gated_rows(back, inner, queries, gain, gate, peers):
    return pl.pallas_call(
        gated_kernel,
        out_shape=jax.ShapeDtypeStruct((peers, *inner.shape), jnp.bfloat16),
        scratch_shapes=[pltpu.VMEM(back.shape, jnp.float32)],
        name="gated",
    )(back, inner, queries, gain[None], gate)


def scan_kernel(chunks, local_ref, before_ref):
    local = local_ref[...].astype(jnp.float32)
    decay = jnp.exp(local[:, 4:8])
    state = local[:, 0:4]
    ahead = [None] * chunks
    run = jnp.zeros((2, 128), jnp.float32)
    for c in range(chunks):
        ahead[c] = run
        run = decay[c, 0:2] * run + state[c, 0:2]
    run = jnp.zeros((2, 128), jnp.float32)
    for c in reversed(range(chunks)):
        before_ref[c] = jnp.concatenate([ahead[c], run], axis=0).astype(jnp.bfloat16)
        run = decay[c, 2:4] * run + state[c, 2:4]


def scanned(arrived):
    chunks = arrived.shape[0]
    return pl.pallas_call(
        lambda *refs: scan_kernel(chunks, *refs),
        out_shape=jax.ShapeDtypeStruct((chunks, 4, 128), jnp.bfloat16),
        name="scan",
    )(arrived)


def gathered_weights(gate, up, down):
    both = jnp.stack([gate, up, down.T])
    first = both[:, :, :HALF]
    second = jnp.pad(both[:, :, HALF:], ((0, 0), (0, 0), (0, 2 * HALF - both.shape[2])))
    halves = jnp.stack([first, second, first, second])
    arrived = lax.all_to_all(halves, ("ya", "yb"), 0, 0, tiled=True)
    shard = jnp.moveaxis(arrived, 0, 1).reshape(3 * 128, HALF)
    return lax.all_gather(shard, "z", axis=0, tiled=True).reshape(-1, 3, 128, HALF)


def exact_terms(x):
    terms = []
    for _ in range(3):
        term = lax.reduce_precision(x, 8, 7)
        terms.append(term.astype(jnp.bfloat16))
        x = x - term
    return terms


SWAP = ((0, 1), (1, 0))


def spread_over_x(output_matrix, residual, gain, bias):
    other = lax.ppermute(residual, "yb", SWAP)
    first = lax.axis_index("yb") == 0
    vectors = jnp.stack(exact_terms(gain) + exact_terms(bias))
    block = jnp.concatenate(
        [
            output_matrix,
            jnp.where(first, residual, other),
            jnp.where(first, other, residual),
            jnp.pad(vectors, ((0, 10), (0, 0))),
        ]
    )
    count = lax.axis_size("x")
    return [block] + [
        lax.ppermute(block, "x", [(i, (i + k) % count) for i in range(count)])
        for k in range(1, count)
    ]


def middle_kernel(place_ref, gated_ref, *refs):
    block_refs, (out_ref, whole_ref, before_ref) = refs[:8], refs[8:]
    heads, rows = 8, gated_ref.shape[2]
    count = 2 * rows
    for core in range(2):
        for pair in range(2):
            for x in range(4):
                head = 2 * x + core
                whole_ref[pair * rows : (pair + 1) * rows, 128 * head : 128 * head + 128] = (
                    gated_ref[core, 4 * pair + x]
                )
    whole = whole_ref[...]
    inner = whole.shape[1]
    total = jnp.zeros((count, 1), jnp.float32)
    for b in range(heads):
        mixer = jnp.dot(whole, block_refs[b][:inner], preferred_element_type=jnp.float32)
        residual = block_refs[b][inner : inner + count].astype(jnp.float32)
        before = alpha_mix * residual + mixer
        before_ref[b] = before
        total = total + jnp.sum(before, axis=1, keepdims=True)
    mean = total / D
    spread = jnp.zeros((count, 1), jnp.float32)
    for b in range(heads):
        centre = before_ref[b] - mean
        spread = spread + jnp.sum(centre * centre, axis=1, keepdims=True)
    scale = lax.rsqrt(spread / D + norm_eps)
    for b in range(heads):
        vectors = block_refs[b][inner + count : inner + count + 16].astype(jnp.float32)
        gain = vectors[0:1] + vectors[1:2] + vectors[2:3]
        bias = vectors[3:4] + vectors[4:5] + vectors[5:6]
        normed = (before_ref[b] - mean) * scale * gain + bias
        out_ref[place_ref[b]] = normed.astype(jnp.bfloat16)


def middle_rows(gated, blocks):
    rows, width = gated.shape[2], blocks[0].shape[1]
    x, core = lax.axis_index("x"), lax.axis_index("c")
    place = jnp.stack([2 * ((x - b // 2 + 4) % 4) + (core + b) % 2 for b in range(8)])
    vmem = pl.BlockSpec(memory_space=pltpu.VMEM)
    return pl.pallas_call(
        middle_kernel,
        in_specs=[pl.BlockSpec(memory_space=pltpu.SMEM)] + [vmem] * 9,
        out_specs=vmem,
        out_shape=jax.ShapeDtypeStruct((8, 2 * rows, width), jnp.bfloat16),
        scratch_shapes=[
            pltpu.VMEM((2 * rows, 8 * 128), jnp.bfloat16),
            pltpu.VMEM((8, 2 * rows, width), jnp.float32),
        ],
        name="middle",
    )(place.astype(jnp.int32), gated, *blocks)


def leaving(hidden, down):
    wide = down.reshape(-1, down.shape[-1])
    return lax.dot_general(
        hidden, wide, (((1,), (1,)), ((), ())), preferred_element_type=jnp.float32
    )


def enter_kernel(
    core_ref, rows_ref, weights_ref, send_ref, hidden_ref, enter_ref, leave_ref, enter_sem, leave_sem
):
    parts, blocks = 4, 4
    each = enter_ref.shape[0] // parts
    copies = []
    for s in range(parts):
        copies.append(
            pltpu.make_async_copy(
                weights_ref.at[pl.ds(s * each, each), pl.ds(0, 2)],
                enter_ref.at[pl.ds(s * each, each)],
                enter_sem.at[s],
            )
        )
    for copy in copies:
        copy.start()
    other = 1 - core_ref[0]
    downs = []
    for s in range(blocks):
        downs.append(
            pltpu.make_async_copy(
                weights_ref.at[pl.ds(4 * s + 2 * other, 2), 2],
                leave_ref.at[pl.ds(2 * s, 2)],
                leave_sem.at[s],
            )
        )
    for copy in downs:
        copy.start()
    gate = up = 0.0
    for s in range(parts):
        x = jnp.concatenate([rows_ref[2 * s], rows_ref[2 * s + 1]], axis=1)
        copies[s].wait()
        wide = [enter_ref[s * each : (s + 1) * each, kind].reshape(-1, HALF) for kind in range(2)]
        gate += jnp.dot(x, wide[0], preferred_element_type=jnp.float32)
        up += jnp.dot(x, wide[1], preferred_element_type=jnp.float32)
    hidden = (gate / (1.0 + jnp.exp(-gate)) * up).astype(jnp.bfloat16)
    hidden_ref[...] = hidden
    rows = send_ref.shape[2]
    for s in range(blocks):
        downs[s].wait()
        product = leaving(hidden, leave_ref[2 * s : 2 * s + 2]).astype(jnp.bfloat16)
        send_ref[0, s] = product[:rows]
        send_ref[1, s] = product[rows:]


def leave_kernel(core_ref, other_ref, hidden_ref, weights_ref, out_ref, leave_ref, leave_sem):
    blocks = 4
    copies = []
    for s in range(blocks):
        copies.append(
            pltpu.make_async_copy(
                weights_ref.at[pl.ds(4 * s + 2 * core_ref[0], 2), 2],
                leave_ref.at[pl.ds(2 * s, 2)],
                leave_sem.at[s],
            )
        )
    for copy in copies:
        copy.start()
    hidden = hidden_ref[...]
    rows = out_ref.shape[2]
    for s in range(blocks):
        copies[s].wait()
        product = leaving(hidden, leave_ref[2 * s : 2 * s + 2])
        for pair in range(2):
            mine = product[pair * rows : (pair + 1) * rows]
            out_ref[pair, s] = (mine + other_ref[pair, s].astype(jnp.float32)).astype(jnp.bfloat16)


SMEM = pl.BlockSpec(memory_space=pltpu.SMEM)
VMEM = pl.BlockSpec(memory_space=pltpu.VMEM)
ANY = pl.BlockSpec(memory_space=pl.ANY)


def feed_enter(core, rows, weights):
    blocks, count, width = rows.shape
    return pl.pallas_call(
        enter_kernel,
        in_specs=[SMEM, VMEM, ANY],
        out_specs=[VMEM, VMEM],
        out_shape=[
            jax.ShapeDtypeStruct((2, blocks // 2, count // 2, width), jnp.bfloat16),
            jax.ShapeDtypeStruct((count, HALF), jnp.bfloat16),
        ],
        scratch_shapes=[
            pltpu.VMEM((16, 2, 128, HALF), jnp.bfloat16),
            pltpu.VMEM((8, 128, HALF), jnp.bfloat16),
            pltpu.SemaphoreType.DMA((4,)),
            pltpu.SemaphoreType.DMA((4,)),
        ],
        cost_estimate=pl.CostEstimate(
            flops=5 * count * D * HALF, bytes_accessed=5 * D * HALF, transcendentals=count * HALF
        ),
        name="feed_enter",
    )(core, rows, weights)


def feed_leave(core, other, hidden, weights):
    return pl.pallas_call(
        leave_kernel,
        in_specs=[SMEM, VMEM, VMEM, ANY],
        out_specs=VMEM,
        out_shape=jax.ShapeDtypeStruct(other.shape, jnp.bfloat16),
        scratch_shapes=[
            pltpu.VMEM((8, 128, HALF), jnp.bfloat16),
            pltpu.SemaphoreType.DMA((4,)),
        ],
        cost_estimate=pl.CostEstimate(
            flops=hidden.shape[0] * D * HALF, bytes_accessed=D * HALF, transcendentals=0
        ),
        name="feed_leave",
    )(core, other, hidden, weights)


def diagonal_of(rows):
    at = lax.broadcasted_iota(jnp.int32, (rows, rows), 0)
    return (at == lax.broadcasted_iota(jnp.int32, (rows, rows), 1)).astype(jnp.float32)


def total_kernel(arrived_ref, own_ref, before_ref, moments_ref):
    feed = arrived_ref[0].astype(jnp.float32)
    for peer in range(1, arrived_ref.shape[0]):
        feed = feed + arrived_ref[peer].astype(jnp.float32)
    before = alpha_mix * own_ref[...].astype(jnp.float32) + feed
    before_ref[...] = before
    diagonal = diagonal_of(before.shape[0])
    moments = []
    for value in (before, before * before):
        column = jnp.sum(value, axis=1, keepdims=True)
        moments.append(jnp.sum(diagonal * column, axis=0, keepdims=True))
    moments = jnp.concatenate(moments, axis=1)
    for peer in range(moments_ref.shape[0]):
        moments_ref[peer] = moments


def closing_kernel(moments_ref, before_ref, gain_ref, bias_ref, out_ref):
    moments = moments_ref[0]
    for peer in range(1, moments_ref.shape[0]):
        moments = moments + moments_ref[peer]
    rows = before_ref.shape[0]
    mean = moments[:, :rows] / D
    spread = moments[:, rows:] / D - mean * mean
    diagonal = diagonal_of(rows)
    column = jnp.sum(diagonal * mean, axis=1, keepdims=True)
    factor = jnp.sum(diagonal * lax.rsqrt(spread + norm_eps), axis=1, keepdims=True)
    out_ref[...] = ((before_ref[...] - column) * factor * gain_ref[...] + bias_ref[...]).astype(
        jnp.bfloat16
    )


def layer(
    query_logits,
    value_rows,
    onward_forget_logits,
    reverse_forget_logits,
    output_gate_logits,
    onward_floor_gap,
    reverse_floor_gap,
    extra_log_decay,
    per_head_gain,
    residual,
    output_matrix,
    inner_norm_gain,
    inner_norm_bias,
    gate_matrix,
    up_matrix,
    down_matrix,
    closing_norm_gain,
    closing_norm_bias,
):
    weights = gathered_weights(gate_matrix, up_matrix, down_matrix)
    rows = query_logits.shape[0]
    inner, queries, packed = local_pass(
        query_logits,
        value_rows,
        onward_forget_logits,
        reverse_forget_logits,
        onward_floor_gap,
        reverse_floor_gap,
        extra_log_decay,
    )
    packed, output_matrix, residual = lax.optimization_barrier((packed, output_matrix, residual))
    arrived = lax.all_to_all(packed, SP, 0, 0, tiled=True)
    blocks = spread_over_x(output_matrix, residual, inner_norm_gain, inner_norm_bias)
    before = scanned(arrived)
    back = lax.all_to_all(before, SP, 0, 0, tiled=True)
    gated = gated_rows(back, inner, queries, per_head_gain, output_gate_logits, 8)
    everyone = lax.all_to_all(gated, ("yb", "x"), 0, 0, tiled=True)
    everyone = lax.all_gather(everyone, "c")
    both = []
    for block in blocks:
        both += [block, lax.ppermute(block, "c", SWAP)]
    middle = middle_rows(everyone, both)
    core = lax.axis_index("c").astype(jnp.int32)[None]
    send, hidden = feed_enter(core, middle, weights)
    joined = feed_leave(core, lax.ppermute(send, "c", SWAP), hidden, weights)
    joined = joined.reshape(-1, *joined.shape[2:])
    shares = lax.all_to_all(joined, ("yb", "x"), 0, 0, tiled=True)
    own = lax.dynamic_slice(
        middle,
        (lax.axis_index(TP), lax.axis_index("yb") * rows, 0),
        (1, rows, middle.shape[2]),
    )[0]
    before_final, moments = pl.pallas_call(
        total_kernel,
        out_shape=[
            jax.ShapeDtypeStruct(own.shape, jnp.float32),
            jax.ShapeDtypeStruct((8, 1, 2 * rows), jnp.float32),
        ],
        name="total",
    )(shares, own)
    return pl.pallas_call(
        closing_kernel,
        out_shape=jax.ShapeDtypeStruct(own.shape, jnp.bfloat16),
        name="closing",
    )(
        lax.all_to_all(moments, TP, 0, 0, tiled=True),
        before_final,
        closing_norm_gain[None],
        closing_norm_bias[None],
    )


def solution(mesh):
    torus = Mesh(mesh.devices.reshape(16, 2, 2, 4, 2), ("z", "ya", "yb", "x", "c"))
    in_specs = (
        P(SP, TP),
        P(SP, TP),
        P(SP, TP),
        P(SP, TP),
        P(SP, TP),
        P(TP),
        P(TP),
        P(SP, TP),
        P(),
        P(SP, TP),
        P(None, TP),
        P(TP),
        P(TP),
        P(SP, TP),
        P(SP, TP),
        P(TP, SP),
        P(TP),
        P(TP),
    )
    out_specs = P(SP, TP)
    return jax.shard_map(layer, mesh=torus, in_specs=in_specs, out_specs=out_specs, check_vma=False)
```

```python
import jax
import jax.numpy as jnp
from jax import lax
from jax.experimental import pallas as pl
from jax.experimental.pallas import tpu as pltpu
from jax.sharding import Mesh
from jax.sharding import PartitionSpec as P


D = 2048
SP = ("z", "ya", "yb")
TP = ("x", "c")
HALF = 384
QUARTER = 32

highest_precision = lax.Precision.HIGHEST
alpha_mix = 2.0**0.25
norm_eps = 1e-05
head_eps = 1e-06


def exact_dot(a, b, dims=((1,), (0,))):
    return lax.dot_general(
        a, b, (dims, ((), ())), precision=highest_precision, preferred_element_type=jnp.float32
    )


def two_terms(x):
    high = x.astype(jnp.bfloat16).astype(jnp.float32)
    return high, (x - high).astype(jnp.bfloat16).astype(jnp.float32)


def local_kernel(
    query_ref,
    value_ref,
    onward_ref,
    reverse_ref,
    onward_gap_ref,
    reverse_gap_ref,
    extra_ref,
    inner_ref,
    queries_ref,
    packed_ref,
    rows_ref,
):
    rows, width = query_ref.shape
    logits = query_ref[...].astype(jnp.float32)
    query = logits / (1.0 + jnp.exp(-logits))
    values = value_ref[...].astype(jnp.float32)
    extra = extra_ref[...]
    at = lax.broadcasted_iota(jnp.int32, (rows, rows), 0)
    source = lax.broadcasted_iota(jnp.int32, (rows, rows), 1)
    ones = jnp.ones((rows, width), jnp.float32)
    inner = jnp.zeros_like(query)
    rows_ref[:, 2 * QUARTER :, :] = jnp.zeros((4, 8, width), jnp.float32)
    for side, (forget_ref, gap_ref, seen, last) in enumerate(
        (
            (onward_ref, onward_gap_ref, at >= source, rows - 1),
            (reverse_ref, reverse_gap_ref, at <= source, 0),
        )
    ):
        seen = seen.astype(jnp.float32)
        keys = gap_ref[...] / (1.0 + jnp.exp(forget_ref[...].astype(jnp.float32)))
        running = exact_dot(seen, jnp.log1p(-keys)) + exact_dot(seen * extra, ones)
        total = running[last : last + 1]
        decayed_query = query * jnp.exp(running)
        scores = exact_dot(decayed_query, keys * jnp.exp(-running), ((1,), (1,))) * seen
        inner = inner + exact_dot(scores, values)
        queries_ref[:, width * side : width * (side + 1)] = decayed_query
        state = exact_dot(values, keys * jnp.exp(total - running), ((0,), (0,)))
        terms = two_terms(total)
        for y in range(4):
            rows_ref[y, QUARTER * side : QUARTER * (side + 1), :] = state[
                QUARTER * y : QUARTER * (y + 1)
            ]
            for t in range(2):
                at_row = 2 * QUARTER + 2 * side + t
                rows_ref[y, at_row : at_row + 1, :] = terms[t]
    packed_ref[...] = rows_ref[...].astype(jnp.bfloat16)
    inner_ref[...] = inner


def near(*arrays):
    return [pltpu.with_memory_space_constraint(a, pltpu.VMEM) for a in arrays]


def local_pass(*arrays):
    rows, width = arrays[0].shape
    return pl.pallas_call(
        local_kernel,
        out_shape=[
            pltpu.VMEM((rows, width), jnp.float32),
            pltpu.VMEM((rows, 2 * width), jnp.float32),
            pltpu.VMEM((4, 2 * QUARTER + 8, width), jnp.bfloat16),
        ],
        scratch_shapes=[pltpu.VMEM((4, 2 * QUARTER + 8, width), jnp.float32)],
        compiler_params=pltpu.CompilerParams(vmem_limit_bytes=6 << 20),
        name="local",
    )(*near(*arrays))


def plane_parts(arrived_ref):
    parts = []
    for side in range(2):
        part = []
        for y in range(4):
            block = arrived_ref[y].astype(jnp.float32)
            decay = block[2 * QUARTER + 2 * side : 2 * QUARTER + 2 * side + 1]
            decay = decay + block[2 * QUARTER + 2 * side + 1 : 2 * QUARTER + 2 * side + 2]
            part.append((decay, block[QUARTER * side : QUARTER * (side + 1)]))
        parts.append(part)
    return parts


def plane_kernel(z_ref, arrived_ref, out_ref, rows_ref):
    forward, backward = plane_parts(arrived_ref)
    wholes = []
    for part in (forward, backward[::-1]):
        decay, state = part[0]
        for next_decay, next_state in part[1:]:
            decay, state = decay + next_decay, jnp.exp(next_decay) * state + next_state
        wholes.append((decay, state))
    for side, (decay, state) in enumerate(wholes):
        rows_ref[side] = jnp.zeros(rows_ref.shape[1:], jnp.float32)
        rows_ref[side, :QUARTER, :] = state
        for t, term in enumerate(two_terms(decay)):
            rows_ref[side, QUARTER + t : QUARTER + t + 1, :] = term
    ahead, behind = rows_ref[0].astype(jnp.bfloat16), rows_ref[1].astype(jnp.bfloat16)
    z = z_ref[0]
    for other in range(out_ref.shape[0]):

        @pl.when(other > z)
        def _():
            out_ref[other] = ahead

        @pl.when(other <= z)
        def _():
            out_ref[other] = behind


def before_kernel(z_ref, planes_ref, arrived_ref, out_ref):
    z = z_ref[0]
    planes = planes_ref.shape[0]
    width = planes_ref.shape[2]
    states = []
    for order in (range(planes), reversed(range(planes))):
        state = jnp.zeros((QUARTER, width), jnp.float32)
        for other in order:
            block = planes_ref[other].astype(jnp.float32)
            decay = block[QUARTER : QUARTER + 1] + block[QUARTER + 1 : QUARTER + 2]
            passed = other < z if not states else other > z
            state = jnp.where(passed, jnp.exp(decay) * state + block[:QUARTER], state)
        states.append(state)
    forward, backward = plane_parts(arrived_ref)
    for side, part in enumerate((forward, backward)):
        state = states[side]
        for y in range(4) if side == 0 else reversed(range(4)):
            out_ref[y, QUARTER * side : QUARTER * (side + 1)] = state.astype(jnp.bfloat16)
            decay, own = part[y]
            state = jnp.exp(decay) * state + own


def states_around(packed):
    z = lax.axis_index("z").astype(jnp.int32)[None]
    planes = lax.axis_size("z")
    width = packed.shape[2]
    (arrived,) = near(lax.all_to_all(packed, ("ya", "yb"), 0, 0, tiled=True))
    totals = pl.pallas_call(
        plane_kernel,
        in_specs=[SMEM, VMEM],
        out_specs=VMEM,
        out_shape=pltpu.VMEM((planes, QUARTER + 8, width), jnp.bfloat16),
        scratch_shapes=[pltpu.VMEM((2, QUARTER + 8, width), jnp.float32)],
        compiler_params=pltpu.CompilerParams(vmem_limit_bytes=4 << 20),
        name="plane",
    )(z, arrived)
    (others,) = near(lax.all_to_all(totals, "z", 0, 0, tiled=True))
    before = pl.pallas_call(
        before_kernel,
        in_specs=[SMEM, VMEM, VMEM],
        out_specs=VMEM,
        out_shape=pltpu.VMEM((4, 2 * QUARTER, width), jnp.bfloat16),
        compiler_params=pltpu.CompilerParams(vmem_limit_bytes=4 << 20),
        name="before",
    )(z, others, arrived)
    return lax.all_to_all(before, ("ya", "yb"), 0, 0, tiled=True)


def gated_kernel(back_ref, inner_ref, queries_ref, gain_ref, gate_ref, out_ref):
    width = inner_ref.shape[1]
    mixed = inner_ref[...]
    for side in range(2):
        state = [back_ref[y, QUARTER * side : QUARTER * (side + 1)] for y in range(4)]
        state = jnp.concatenate([part.astype(jnp.float32) for part in state], axis=0)
        queries = queries_ref[:, width * side : width * (side + 1)]
        mixed = mixed + exact_dot(queries, state, ((1,), (1,)))
    mean = jnp.mean(mixed * mixed, axis=1, keepdims=True)
    normed = mixed * lax.rsqrt(mean + head_eps) * gain_ref[...]
    gate = gate_ref[...].astype(jnp.float32)
    gated = (normed * (gate / (1.0 + jnp.exp(-gate)))).astype(jnp.bfloat16)
    for peer in range(out_ref.shape[0]):
        out_ref[peer] = gated


def gated_rows(*arrays):
    return pl.pallas_call(
        gated_kernel,
        out_shape=pltpu.VMEM((8, *arrays[1].shape), jnp.bfloat16),
        compiler_params=pltpu.CompilerParams(vmem_limit_bytes=4 << 20),
        name="gated",
    )(*near(*arrays))


SMEM = pl.BlockSpec(memory_space=pltpu.SMEM)
VMEM = pl.BlockSpec(memory_space=pltpu.VMEM)
ANY = pl.BlockSpec(memory_space=pl.ANY)


def gathered_weights(gate, up, down):
    both = jnp.stack([gate, up, down.T])
    first = both[:, :, :HALF]
    second = jnp.pad(both[:, :, HALF:], ((0, 0), (0, 0), (0, 2 * HALF - both.shape[2])))
    halves = jnp.stack([first, second, first, second])
    arrived = lax.all_to_all(halves, ("ya", "yb"), 0, 0, tiled=True)
    shard = jnp.moveaxis(arrived, 0, 1).reshape(3 * 128, HALF)
    weights = lax.all_gather(shard, "z", axis=0, tiled=True).reshape(-1, 3, 128, HALF)
    return pltpu.with_memory_space_constraint(weights, pltpu.HBM)


def exact_terms(x):
    terms = []
    for _ in range(3):
        term = lax.reduce_precision(x, 8, 7)
        terms.append(term.astype(jnp.bfloat16))
        x = x - term
    return terms


SWAP = ((0, 1), (1, 0))


def spread_over_x(output_matrix, residual, gain, bias):
    other = lax.ppermute(residual, "yb", SWAP)
    first = lax.axis_index("yb") == 0
    vectors = jnp.stack(exact_terms(gain) + exact_terms(bias))
    block = jnp.concatenate(
        [
            output_matrix,
            jnp.where(first, residual, other),
            jnp.where(first, other, residual),
            jnp.pad(vectors, ((0, 10), (0, 0))),
        ]
    )
    count = lax.axis_size("x")
    return [block] + [
        lax.ppermute(block, "x", [(i, (i + k) % count) for i in range(count)])
        for k in range(1, count)
    ]


def middle_kernel(place_ref, gated_ref, *refs):
    block_refs, (out_ref, whole_ref, before_ref) = refs[:8], refs[8:]
    heads, rows = 8, gated_ref.shape[2]
    count = 2 * rows
    for core in range(2):
        for pair in range(2):
            for x in range(4):
                head = 2 * x + core
                whole_ref[pair * rows : (pair + 1) * rows, 128 * head : 128 * head + 128] = (
                    gated_ref[core, 4 * pair + x]
                )
    whole = whole_ref[...]
    inner = whole.shape[1]
    total = jnp.zeros((count, 1), jnp.float32)
    for b in range(heads):
        mixer = jnp.dot(whole, block_refs[b][:inner], preferred_element_type=jnp.float32)
        residual = block_refs[b][inner : inner + count].astype(jnp.float32)
        before = alpha_mix * residual + mixer
        before_ref[b] = before
        total = total + jnp.sum(before, axis=1, keepdims=True)
    mean = total / D
    spread = jnp.zeros((count, 1), jnp.float32)
    for b in range(heads):
        centre = before_ref[b] - mean
        spread = spread + jnp.sum(centre * centre, axis=1, keepdims=True)
    scale = lax.rsqrt(spread / D + norm_eps)
    for b in range(heads):
        vectors = block_refs[b][inner + count : inner + count + 16].astype(jnp.float32)
        gain = vectors[0:1] + vectors[1:2] + vectors[2:3]
        bias = vectors[3:4] + vectors[4:5] + vectors[5:6]
        normed = (before_ref[b] - mean) * scale * gain + bias
        out_ref[place_ref[b]] = normed.astype(jnp.bfloat16)


def middle_rows(gated, blocks):
    rows, width = gated.shape[2], blocks[0].shape[1]
    x, core = lax.axis_index("x"), lax.axis_index("c")
    place = jnp.stack([2 * ((x - b // 2 + 4) % 4) + (core + b) % 2 for b in range(8)])
    vmem = pl.BlockSpec(memory_space=pltpu.VMEM)
    return pl.pallas_call(
        middle_kernel,
        in_specs=[pl.BlockSpec(memory_space=pltpu.SMEM)] + [vmem] * 9,
        out_specs=vmem,
        out_shape=pltpu.VMEM((8, 2 * rows, width), jnp.bfloat16),
        scratch_shapes=[
            pltpu.VMEM((2 * rows, 8 * 128), jnp.bfloat16),
            pltpu.VMEM((8, 2 * rows, width), jnp.float32),
        ],
        compiler_params=pltpu.CompilerParams(vmem_limit_bytes=14 << 20),
        name="middle",
    )(place.astype(jnp.int32), *near(gated), *blocks)


def leaving(hidden, down):
    wide = down.reshape(-1, down.shape[-1])
    return lax.dot_general(
        hidden, wide, (((1,), (1,)), ((), ())), preferred_element_type=jnp.float32
    )


def enter_kernel(
    core_ref, rows_ref, weights_ref, send_ref, hidden_ref, enter_ref, leave_ref, enter_sem, leave_sem
):
    parts, blocks = 4, 4
    each = enter_ref.shape[0] // parts
    copies = []
    for s in range(parts):
        copies.append(
            pltpu.make_async_copy(
                weights_ref.at[pl.ds(s * each, each), pl.ds(0, 2)],
                enter_ref.at[pl.ds(s * each, each)],
                enter_sem.at[s],
            )
        )
    for copy in copies:
        copy.start()
    other = 1 - core_ref[0]
    downs = []
    for s in range(blocks):
        downs.append(
            pltpu.make_async_copy(
                weights_ref.at[pl.ds(4 * s + 2 * other, 2), 2],
                leave_ref.at[pl.ds(2 * s, 2)],
                leave_sem.at[s],
            )
        )
    for copy in downs:
        copy.start()
    gate = up = 0.0
    for s in range(parts):
        x = jnp.concatenate([rows_ref[2 * s], rows_ref[2 * s + 1]], axis=1)
        copies[s].wait()
        wide = [enter_ref[s * each : (s + 1) * each, kind].reshape(-1, HALF) for kind in range(2)]
        gate += jnp.dot(x, wide[0], preferred_element_type=jnp.float32)
        up += jnp.dot(x, wide[1], preferred_element_type=jnp.float32)
    hidden = (gate / (1.0 + jnp.exp(-gate)) * up).astype(jnp.bfloat16)
    hidden_ref[...] = hidden
    rows = send_ref.shape[2]
    for s in range(blocks):
        downs[s].wait()
        product = leaving(hidden, leave_ref[2 * s : 2 * s + 2]).astype(jnp.bfloat16)
        send_ref[0, s] = product[:rows]
        send_ref[1, s] = product[rows:]


def leave_kernel(core_ref, other_ref, hidden_ref, weights_ref, out_ref, leave_ref, leave_sem):
    blocks = 4
    copies = []
    for s in range(blocks):
        copies.append(
            pltpu.make_async_copy(
                weights_ref.at[pl.ds(4 * s + 2 * core_ref[0], 2), 2],
                leave_ref.at[pl.ds(2 * s, 2)],
                leave_sem.at[s],
            )
        )
    for copy in copies:
        copy.start()
    hidden = hidden_ref[...]
    rows = out_ref.shape[2]
    for s in range(blocks):
        copies[s].wait()
        product = leaving(hidden, leave_ref[2 * s : 2 * s + 2])
        for pair in range(2):
            mine = product[pair * rows : (pair + 1) * rows]
            out_ref[pair, s] = (mine + other_ref[pair, s].astype(jnp.float32)).astype(jnp.bfloat16)


def feed_enter(core, rows, weights):
    blocks, count, width = rows.shape
    return pl.pallas_call(
        enter_kernel,
        in_specs=[SMEM, VMEM, ANY],
        out_specs=[VMEM, VMEM],
        out_shape=[
            pltpu.VMEM((2, blocks // 2, count // 2, width), jnp.bfloat16),
            pltpu.VMEM((count, HALF), jnp.bfloat16),
        ],
        scratch_shapes=[
            pltpu.VMEM((16, 2, 128, HALF), jnp.bfloat16),
            pltpu.VMEM((8, 128, HALF), jnp.bfloat16),
            pltpu.SemaphoreType.DMA((4,)),
            pltpu.SemaphoreType.DMA((4,)),
        ],
        cost_estimate=pl.CostEstimate(
            flops=5 * count * D * HALF, bytes_accessed=5 * D * HALF, transcendentals=count * HALF
        ),
        compiler_params=pltpu.CompilerParams(vmem_limit_bytes=16 << 20),
        name="feed_enter",
    )(core, *near(rows), weights)


def feed_leave(core, other, hidden, weights):
    return pl.pallas_call(
        leave_kernel,
        in_specs=[SMEM, VMEM, VMEM, ANY],
        out_specs=VMEM,
        out_shape=pltpu.VMEM(other.shape, jnp.bfloat16),
        scratch_shapes=[
            pltpu.VMEM((8, 128, HALF), jnp.bfloat16),
            pltpu.SemaphoreType.DMA((4,)),
        ],
        cost_estimate=pl.CostEstimate(
            flops=hidden.shape[0] * D * HALF, bytes_accessed=D * HALF, transcendentals=0
        ),
        compiler_params=pltpu.CompilerParams(vmem_limit_bytes=8 << 20),
        name="feed_leave",
    )(core, *near(other, hidden), weights)


def diagonal_of(rows):
    at = lax.broadcasted_iota(jnp.int32, (rows, rows), 0)
    return (at == lax.broadcasted_iota(jnp.int32, (rows, rows), 1)).astype(jnp.float32)


def total_kernel(arrived_ref, own_ref, before_ref, moments_ref):
    feed = arrived_ref[0].astype(jnp.float32)
    for peer in range(1, arrived_ref.shape[0]):
        feed = feed + arrived_ref[peer].astype(jnp.float32)
    before = alpha_mix * own_ref[...].astype(jnp.float32) + feed
    before_ref[...] = before
    diagonal = diagonal_of(before.shape[0])
    moments = []
    for value in (before, before * before):
        column = jnp.sum(value, axis=1, keepdims=True)
        moments.append(jnp.sum(diagonal * column, axis=0, keepdims=True))
    moments = jnp.concatenate(moments, axis=1)
    for peer in range(moments_ref.shape[0]):
        moments_ref[peer] = moments


def closing_kernel(moments_ref, before_ref, gain_ref, bias_ref, out_ref):
    moments = moments_ref[0]
    for peer in range(1, moments_ref.shape[0]):
        moments = moments + moments_ref[peer]
    rows = before_ref.shape[0]
    mean = moments[:, :rows] / D
    spread = moments[:, rows:] / D - mean * mean
    diagonal = diagonal_of(rows)
    column = jnp.sum(diagonal * mean, axis=1, keepdims=True)
    factor = jnp.sum(diagonal * lax.rsqrt(spread + norm_eps), axis=1, keepdims=True)
    out_ref[...] = ((before_ref[...] - column) * factor * gain_ref[...] + bias_ref[...]).astype(
        jnp.bfloat16
    )


def layer(
    query_logits,
    value_rows,
    onward_forget_logits,
    reverse_forget_logits,
    output_gate_logits,
    onward_floor_gap,
    reverse_floor_gap,
    extra_log_decay,
    per_head_gain,
    residual,
    output_matrix,
    inner_norm_gain,
    inner_norm_bias,
    gate_matrix,
    up_matrix,
    down_matrix,
    closing_norm_gain,
    closing_norm_bias,
):
    weights = gathered_weights(gate_matrix, up_matrix, down_matrix)
    rows = query_logits.shape[0]
    inner, queries, packed = local_pass(
        query_logits,
        value_rows,
        onward_forget_logits,
        reverse_forget_logits,
        onward_floor_gap[None],
        reverse_floor_gap[None],
        extra_log_decay.reshape(1, rows),
    )
    packed, output_matrix, residual = lax.optimization_barrier((packed, output_matrix, residual))
    back = states_around(packed)
    blocks = spread_over_x(output_matrix, residual, inner_norm_gain, inner_norm_bias)
    gated = gated_rows(back, inner, queries, per_head_gain[None], output_gate_logits)
    everyone = lax.all_to_all(gated, ("yb", "x"), 0, 0, tiled=True)
    everyone = lax.all_gather(everyone, "c")
    both = []
    for block in blocks:
        both += [block, lax.ppermute(block, "c", SWAP)]
    middle = middle_rows(everyone, both)
    core = lax.axis_index("c").astype(jnp.int32)[None]
    send, hidden = feed_enter(core, middle, weights)
    joined = feed_leave(core, lax.ppermute(send, "c", SWAP), hidden, weights)
    joined = joined.reshape(-1, *joined.shape[2:])
    shares = lax.all_to_all(joined, ("yb", "x"), 0, 0, tiled=True)
    own = lax.dynamic_slice(
        middle,
        (lax.axis_index(TP), lax.axis_index("yb") * rows, 0),
        (1, rows, middle.shape[2]),
    )[0]
    before_final, moments = pl.pallas_call(
        total_kernel,
        out_shape=[
            pltpu.VMEM(own.shape, jnp.float32),
            pltpu.VMEM((8, 1, 2 * rows), jnp.float32),
        ],
        compiler_params=pltpu.CompilerParams(vmem_limit_bytes=4 << 20),
        name="total",
    )(*near(shares, own))
    moments = lax.all_to_all(moments, TP, 0, 0, tiled=True)
    return pl.pallas_call(
        closing_kernel,
        out_shape=jax.ShapeDtypeStruct(own.shape, jnp.bfloat16),
        compiler_params=pltpu.CompilerParams(vmem_limit_bytes=4 << 20),
        name="closing",
    )(*near(moments, before_final, closing_norm_gain[None], closing_norm_bias[None]))


def solution(mesh):
    torus = Mesh(mesh.devices.reshape(16, 2, 2, 4, 2), ("z", "ya", "yb", "x", "c"))
    in_specs = (
        P(SP, TP),
        P(SP, TP),
        P(SP, TP),
        P(SP, TP),
        P(SP, TP),
        P(TP),
        P(TP),
        P(SP, TP),
        P(),
        P(SP, TP),
        P(None, TP),
        P(TP),
        P(TP),
        P(SP, TP),
        P(SP, TP),
        P(TP, SP),
        P(TP),
        P(TP),
    )
    out_specs = P(SP, TP)
    return jax.shard_map(layer, mesh=torus, in_specs=in_specs, out_specs=out_specs, check_vma=False)
```

```python
import jax
import jax.numpy as jnp
from jax import lax
from jax.experimental import pallas as pl
from jax.experimental.pallas import tpu as pltpu
from jax.sharding import Mesh
from jax.sharding import PartitionSpec as P


D = 2048
SP = ("z", "ya", "yb")
TP = ("x", "c")
HALF = 352
QUARTER = 32

highest_precision = lax.Precision.HIGHEST
alpha_mix = 2.0**0.25
norm_eps = 1e-05
head_eps = 1e-06


def exact_dot(a, b, dims=((1,), (0,))):
    return lax.dot_general(
        a, b, (dims, ((), ())), precision=highest_precision, preferred_element_type=jnp.float32
    )


def two_terms(x):
    high = x.astype(jnp.bfloat16).astype(jnp.float32)
    return high, (x - high).astype(jnp.bfloat16).astype(jnp.float32)


def local_kernel(
    query_ref,
    value_ref,
    onward_ref,
    reverse_ref,
    onward_gap_ref,
    reverse_gap_ref,
    extra_ref,
    inner_ref,
    queries_ref,
    packed_ref,
    rows_ref,
):
    rows, width = query_ref.shape
    logits = query_ref[...].astype(jnp.float32)
    query = logits / (1.0 + jnp.exp(-logits))
    values = value_ref[...].astype(jnp.float32)
    extra = extra_ref[...]
    at = lax.broadcasted_iota(jnp.int32, (rows, rows), 0)
    source = lax.broadcasted_iota(jnp.int32, (rows, rows), 1)
    ones = jnp.ones((rows, width), jnp.float32)
    inner = jnp.zeros_like(query)
    rows_ref[:, 2 * QUARTER :, :] = jnp.zeros((4, 8, width), jnp.float32)
    for side, (forget_ref, gap_ref, seen, last) in enumerate(
        (
            (onward_ref, onward_gap_ref, at >= source, rows - 1),
            (reverse_ref, reverse_gap_ref, at <= source, 0),
        )
    ):
        seen = seen.astype(jnp.float32)
        keys = gap_ref[...] / (1.0 + jnp.exp(forget_ref[...].astype(jnp.float32)))
        running = exact_dot(seen, jnp.log1p(-keys)) + exact_dot(seen * extra, ones)
        total = running[last : last + 1]
        decayed_query = query * jnp.exp(running)
        scores = exact_dot(decayed_query, keys * jnp.exp(-running), ((1,), (1,))) * seen
        inner = inner + exact_dot(scores, values)
        queries_ref[:, width * side : width * (side + 1)] = decayed_query
        state = exact_dot(values, keys * jnp.exp(total - running), ((0,), (0,)))
        terms = two_terms(total)
        for y in range(4):
            rows_ref[y, QUARTER * side : QUARTER * (side + 1), :] = state[
                QUARTER * y : QUARTER * (y + 1)
            ]
            for t in range(2):
                at_row = 2 * QUARTER + 2 * side + t
                rows_ref[y, at_row : at_row + 1, :] = terms[t]
    packed_ref[...] = rows_ref[...].astype(jnp.bfloat16)
    inner_ref[...] = inner


def near(*arrays):
    return [pltpu.with_memory_space_constraint(a, pltpu.VMEM) for a in arrays]


def local_pass(*arrays):
    rows, width = arrays[0].shape
    return pl.pallas_call(
        local_kernel,
        out_shape=[
            pltpu.VMEM((rows, width), jnp.float32),
            pltpu.VMEM((rows, 2 * width), jnp.float32),
            pltpu.VMEM((4, 2 * QUARTER + 8, width), jnp.bfloat16),
        ],
        scratch_shapes=[pltpu.VMEM((4, 2 * QUARTER + 8, width), jnp.float32)],
        compiler_params=pltpu.CompilerParams(vmem_limit_bytes=6 << 20),
        name="local",
    )(*near(*arrays))


def plane_parts(arrived_ref):
    parts = []
    for side in range(2):
        part = []
        for y in range(4):
            block = arrived_ref[y].astype(jnp.float32)
            decay = block[2 * QUARTER + 2 * side : 2 * QUARTER + 2 * side + 1]
            decay = decay + block[2 * QUARTER + 2 * side + 1 : 2 * QUARTER + 2 * side + 2]
            part.append((decay, block[QUARTER * side : QUARTER * (side + 1)]))
        parts.append(part)
    return parts


def plane_kernel(z_ref, arrived_ref, out_ref, rows_ref):
    forward, backward = plane_parts(arrived_ref)
    wholes = []
    for part in (forward, backward[::-1]):
        decay, state = part[0]
        for next_decay, next_state in part[1:]:
            decay, state = decay + next_decay, jnp.exp(next_decay) * state + next_state
        wholes.append((decay, state))
    for side, (decay, state) in enumerate(wholes):
        rows_ref[side] = jnp.zeros(rows_ref.shape[1:], jnp.float32)
        rows_ref[side, :QUARTER, :] = state
        for t, term in enumerate(two_terms(decay)):
            rows_ref[side, QUARTER + t : QUARTER + t + 1, :] = term
    ahead, behind = rows_ref[0].astype(jnp.bfloat16), rows_ref[1].astype(jnp.bfloat16)
    z = z_ref[0]
    for other in range(out_ref.shape[0]):

        @pl.when(other > z)
        def _():
            out_ref[other] = ahead

        @pl.when(other <= z)
        def _():
            out_ref[other] = behind


def before_kernel(z_ref, planes_ref, arrived_ref, out_ref):
    z = z_ref[0]
    planes = planes_ref.shape[0]
    width = planes_ref.shape[2]
    states = []
    for order in (range(planes), reversed(range(planes))):
        state = jnp.zeros((QUARTER, width), jnp.float32)
        for other in order:
            block = planes_ref[other].astype(jnp.float32)
            decay = block[QUARTER : QUARTER + 1] + block[QUARTER + 1 : QUARTER + 2]
            passed = other < z if not states else other > z
            state = jnp.where(passed, jnp.exp(decay) * state + block[:QUARTER], state)
        states.append(state)
    forward, backward = plane_parts(arrived_ref)
    for side, part in enumerate((forward, backward)):
        state = states[side]
        for y in range(4) if side == 0 else reversed(range(4)):
            out_ref[y, QUARTER * side : QUARTER * (side + 1)] = state.astype(jnp.bfloat16)
            decay, own = part[y]
            state = jnp.exp(decay) * state + own


def states_around(packed):
    z = lax.axis_index("z").astype(jnp.int32)[None]
    planes = lax.axis_size("z")
    width = packed.shape[2]
    (arrived,) = near(lax.all_to_all(packed, ("ya", "yb"), 0, 0, tiled=True))
    totals = pl.pallas_call(
        plane_kernel,
        in_specs=[SMEM, VMEM],
        out_specs=VMEM,
        out_shape=pltpu.VMEM((planes, QUARTER + 8, width), jnp.bfloat16),
        scratch_shapes=[pltpu.VMEM((2, QUARTER + 8, width), jnp.float32)],
        compiler_params=pltpu.CompilerParams(vmem_limit_bytes=4 << 20),
        name="plane",
    )(z, arrived)
    (others,) = near(lax.all_to_all(totals, "z", 0, 0, tiled=True))
    before = pl.pallas_call(
        before_kernel,
        in_specs=[SMEM, VMEM, VMEM],
        out_specs=VMEM,
        out_shape=pltpu.VMEM((4, 2 * QUARTER, width), jnp.bfloat16),
        compiler_params=pltpu.CompilerParams(vmem_limit_bytes=4 << 20),
        name="before",
    )(z, others, arrived)
    return lax.all_to_all(before, ("ya", "yb"), 0, 0, tiled=True)


def gated_kernel(back_ref, inner_ref, queries_ref, gain_ref, gate_ref, out_ref):
    width = inner_ref.shape[1]
    mixed = inner_ref[...]
    for side in range(2):
        state = [back_ref[y, QUARTER * side : QUARTER * (side + 1)] for y in range(4)]
        state = jnp.concatenate([part.astype(jnp.float32) for part in state], axis=0)
        queries = queries_ref[:, width * side : width * (side + 1)]
        mixed = mixed + exact_dot(queries, state, ((1,), (1,)))
    mean = jnp.mean(mixed * mixed, axis=1, keepdims=True)
    normed = mixed * lax.rsqrt(mean + head_eps) * gain_ref[...]
    gate = gate_ref[...].astype(jnp.float32)
    gated = (normed * (gate / (1.0 + jnp.exp(-gate)))).astype(jnp.bfloat16)
    for peer in range(out_ref.shape[0]):
        out_ref[peer] = gated


def gated_rows(*arrays):
    return pl.pallas_call(
        gated_kernel,
        out_shape=pltpu.VMEM((8, *arrays[1].shape), jnp.bfloat16),
        compiler_params=pltpu.CompilerParams(vmem_limit_bytes=4 << 20),
        name="gated",
    )(*near(*arrays))


SMEM = pl.BlockSpec(memory_space=pltpu.SMEM)
VMEM = pl.BlockSpec(memory_space=pltpu.VMEM)
ANY = pl.BlockSpec(memory_space=pl.ANY)


def turn_kernel(in_ref, out_ref):
    for kind in range(3):
        rows = jnp.concatenate([in_ref[y, kind] for y in range(4)], axis=0)
        out_ref[kind] = rows.T


def gathered_weights(gate, up, down):
    both = jnp.stack([gate, up, down.T])
    halves = [both[:, :, :HALF], both[:, :, HALF:]]
    arrived = lax.all_to_all(jnp.stack(halves + halves), ("ya", "yb"), 0, 0, tiled=True)
    shard = pl.pallas_call(
        turn_kernel,
        out_shape=jax.ShapeDtypeStruct((3, HALF, 128), jnp.bfloat16),
        compiler_params=pltpu.CompilerParams(vmem_limit_bytes=6 << 20),
        name="turn",
    )(*near(arrived)).reshape(3 * HALF, 128)
    weights = lax.all_gather(shard, "z", axis=0, tiled=True).reshape(-1, 3, HALF, 128)
    return pltpu.with_memory_space_constraint(weights, pltpu.HBM)


def exact_terms(x):
    terms = []
    for _ in range(3):
        term = lax.reduce_precision(x, 8, 7)
        terms.append(term.astype(jnp.bfloat16))
        x = x - term
    return terms


SWAP = ((0, 1), (1, 0))


def spread_over_x(output_matrix, residual, gain, bias):
    other = lax.ppermute(residual, "yb", SWAP)
    first = lax.axis_index("yb") == 0
    vectors = jnp.stack(exact_terms(gain) + exact_terms(bias))
    block = jnp.concatenate(
        [
            output_matrix,
            jnp.where(first, residual, other),
            jnp.where(first, other, residual),
            jnp.pad(vectors, ((0, 10), (0, 0))),
        ]
    )
    count = lax.axis_size("x")
    return [block] + [
        lax.ppermute(block, "x", [(i, (i + k) % count) for i in range(count)])
        for k in range(1, count)
    ]


def middle_kernel(place_ref, gated_ref, *refs):
    block_refs, (out_ref, own_ref, whole_ref, before_ref) = refs[:8], refs[8:]
    heads, rows = 8, gated_ref.shape[2]
    count = 2 * rows
    for core in range(2):
        for pair in range(2):
            for x in range(4):
                head = 2 * x + core
                whole_ref[pair * rows : (pair + 1) * rows, 128 * head : 128 * head + 128] = (
                    gated_ref[core, 4 * pair + x]
                )
    whole = whole_ref[...]
    inner = whole.shape[1]
    total = jnp.zeros((count, 1), jnp.float32)
    for b in range(heads):
        mixer = jnp.dot(whole, block_refs[b][:inner], preferred_element_type=jnp.float32)
        residual = block_refs[b][inner : inner + count].astype(jnp.float32)
        before = alpha_mix * residual + mixer
        before_ref[b] = before
        total = total + jnp.sum(before, axis=1, keepdims=True)
    mean = total / D
    spread = jnp.zeros((count, 1), jnp.float32)
    for b in range(heads):
        centre = before_ref[b] - mean
        spread = spread + jnp.sum(centre * centre, axis=1, keepdims=True)
    scale = lax.rsqrt(spread / D + norm_eps)
    for b in range(heads):
        vectors = block_refs[b][inner + count : inner + count + 16].astype(jnp.float32)
        gain = vectors[0:1] + vectors[1:2] + vectors[2:3]
        bias = vectors[3:4] + vectors[4:5] + vectors[5:6]
        normed = (before_ref[b] - mean) * scale * gain + bias
        normed = normed.astype(jnp.bfloat16)
        out_ref[place_ref[b]] = normed
        if b == 0:
            own_ref[...] = jnp.where(place_ref[heads] == 0, normed[:rows], normed[rows:])


def middle_rows(gated, blocks):
    rows, width = gated.shape[2], blocks[0].shape[1]
    x, core = lax.axis_index("x"), lax.axis_index("c")
    place = [2 * ((x - b // 2 + 4) % 4) + (core + b) % 2 for b in range(8)]
    place = jnp.stack(place + [lax.axis_index("yb")])
    vmem = pl.BlockSpec(memory_space=pltpu.VMEM)
    return pl.pallas_call(
        middle_kernel,
        in_specs=[pl.BlockSpec(memory_space=pltpu.SMEM)] + [vmem] * 9,
        out_specs=[vmem, vmem],
        out_shape=[
            pltpu.VMEM((8, 2 * rows, width), jnp.bfloat16),
            pltpu.VMEM((rows, width), jnp.bfloat16),
        ],
        scratch_shapes=[
            pltpu.VMEM((2 * rows, 8 * 128), jnp.bfloat16),
            pltpu.VMEM((8, 2 * rows, width), jnp.float32),
        ],
        compiler_params=pltpu.CompilerParams(vmem_limit_bytes=14 << 20),
        name="middle",
    )(place.astype(jnp.int32), *near(gated), *blocks)


def leaving(hidden, down_ref, block):
    wide = jnp.concatenate([down_ref[2 * block], down_ref[2 * block + 1]], axis=1)
    return jnp.dot(hidden, wide, preferred_element_type=jnp.float32)


def down_copies(core, weights_ref, leave_ref, sem_ref):
    copies = []
    for s in range(4):
        copies.append(
            pltpu.make_async_copy(
                weights_ref.at[pl.ds(4 * s + 2 * core, 2), 2],
                leave_ref.at[pl.ds(2 * s, 2)],
                sem_ref.at[s],
            )
        )
    return copies


def enter_kernel(
    core_ref, rows_ref, weights_ref, send_ref, hidden_ref, enter_ref, leave_ref, enter_sem, leave_sem
):
    parts, each = 4, 4
    copies = []
    for s in range(parts):
        copies.append(
            pltpu.make_async_copy(
                weights_ref.at[pl.ds(s * each, each), pl.ds(0, 2)],
                enter_ref.at[pl.ds(s * each, each)],
                enter_sem.at[s],
            )
        )
    downs = down_copies(1 - core_ref[0], weights_ref, leave_ref, leave_sem)
    for copy in copies + downs:
        copy.start()
    sums = [0.0, 0.0]
    for s in range(parts):
        x = jnp.concatenate([rows_ref[2 * s], rows_ref[2 * s + 1]], axis=1)
        copies[s].wait()
        for kind in range(2):
            wide = [enter_ref[each * s + j, kind] for j in range(each)]
            sums[kind] += lax.dot_general(
                x,
                jnp.concatenate(wide, axis=1),
                (((1,), (1,)), ((), ())),
                preferred_element_type=jnp.float32,
            )
    gate, up = sums
    hidden = (gate / (1.0 + jnp.exp(-gate)) * up).astype(jnp.bfloat16)
    hidden_ref[...] = hidden
    rows = send_ref.shape[2]
    for s in range(4):
        downs[s].wait()
        product = leaving(hidden, leave_ref, s).astype(jnp.bfloat16)
        send_ref[0, s] = product[:rows]
        send_ref[1, s] = product[rows:]


def leave_kernel(core_ref, hidden_ref, weights_ref, out_ref, leave_ref, leave_sem):
    downs = down_copies(core_ref[0], weights_ref, leave_ref, leave_sem)
    for copy in downs:
        copy.start()
    hidden = hidden_ref[...]
    rows = out_ref.shape[2]
    for s in range(4):
        downs[s].wait()
        product = leaving(hidden, leave_ref, s)
        out_ref[0, s] = product[:rows]
        out_ref[1, s] = product[rows:]


def join_kernel(mine_ref, other_ref, out_ref):
    for pair in range(2):
        for s in range(4):
            total = mine_ref[pair, s] + other_ref[pair, s].astype(jnp.float32)
            out_ref[4 * pair + s] = total.astype(jnp.bfloat16)


def feed_enter(core, rows, weights):
    blocks, count, width = rows.shape
    return pl.pallas_call(
        enter_kernel,
        in_specs=[SMEM, VMEM, ANY],
        out_specs=[VMEM, VMEM],
        out_shape=[
            pltpu.VMEM((2, blocks // 2, count // 2, width), jnp.bfloat16),
            pltpu.VMEM((count, HALF), jnp.bfloat16),
        ],
        scratch_shapes=[
            pltpu.VMEM((16, 2, HALF, 128), jnp.bfloat16),
            pltpu.VMEM((8, HALF, 128), jnp.bfloat16),
            pltpu.SemaphoreType.DMA((4,)),
            pltpu.SemaphoreType.DMA((4,)),
        ],
        cost_estimate=pl.CostEstimate(
            flops=5 * count * D * HALF, bytes_accessed=5 * D * HALF, transcendentals=count * HALF
        ),
        compiler_params=pltpu.CompilerParams(vmem_limit_bytes=16 << 20),
        name="feed_enter",
    )(core, *near(rows), weights)


def feed_leave(core, hidden, weights):
    count = hidden.shape[0]
    return pl.pallas_call(
        leave_kernel,
        in_specs=[SMEM, VMEM, ANY],
        out_specs=VMEM,
        out_shape=pltpu.VMEM((2, 4, count // 2, 256), jnp.float32),
        scratch_shapes=[
            pltpu.VMEM((8, HALF, 128), jnp.bfloat16),
            pltpu.SemaphoreType.DMA((4,)),
        ],
        cost_estimate=pl.CostEstimate(
            flops=count * D * HALF, bytes_accessed=D * HALF, transcendentals=0
        ),
        compiler_params=pltpu.CompilerParams(vmem_limit_bytes=8 << 20),
        name="feed_leave",
    )(core, *near(hidden), weights)


def joined(mine, other):
    return pl.pallas_call(
        join_kernel,
        out_shape=pltpu.VMEM((8, *mine.shape[2:]), jnp.bfloat16),
        compiler_params=pltpu.CompilerParams(vmem_limit_bytes=8 << 20),
        name="join",
    )(*near(mine, other))


def diagonal_of(rows):
    at = lax.broadcasted_iota(jnp.int32, (rows, rows), 0)
    return (at == lax.broadcasted_iota(jnp.int32, (rows, rows), 1)).astype(jnp.float32)


def total_kernel(arrived_ref, own_ref, before_ref, moments_ref):
    feed = arrived_ref[0].astype(jnp.float32)
    for peer in range(1, arrived_ref.shape[0]):
        feed = feed + arrived_ref[peer].astype(jnp.float32)
    before = alpha_mix * own_ref[...].astype(jnp.float32) + feed
    before_ref[...] = before
    diagonal = diagonal_of(before.shape[0])
    moments = []
    for value in (before, before * before):
        column = jnp.sum(value, axis=1, keepdims=True)
        moments.append(jnp.sum(diagonal * column, axis=0, keepdims=True))
    moments = jnp.concatenate(moments, axis=1)
    for peer in range(moments_ref.shape[0]):
        moments_ref[peer] = moments


def closing_kernel(moments_ref, before_ref, gain_ref, bias_ref, out_ref):
    moments = moments_ref[0]
    for peer in range(1, moments_ref.shape[0]):
        moments = moments + moments_ref[peer]
    rows = before_ref.shape[0]
    mean = moments[:, :rows] / D
    spread = moments[:, rows:] / D - mean * mean
    diagonal = diagonal_of(rows)
    column = jnp.sum(diagonal * mean, axis=1, keepdims=True)
    factor = jnp.sum(diagonal * lax.rsqrt(spread + norm_eps), axis=1, keepdims=True)
    out_ref[...] = ((before_ref[...] - column) * factor * gain_ref[...] + bias_ref[...]).astype(
        jnp.bfloat16
    )


def layer(
    query_logits,
    value_rows,
    onward_forget_logits,
    reverse_forget_logits,
    output_gate_logits,
    onward_floor_gap,
    reverse_floor_gap,
    extra_log_decay,
    per_head_gain,
    residual,
    output_matrix,
    inner_norm_gain,
    inner_norm_bias,
    gate_matrix,
    up_matrix,
    down_matrix,
    closing_norm_gain,
    closing_norm_bias,
):
    weights = gathered_weights(gate_matrix, up_matrix, down_matrix)
    rows = query_logits.shape[0]
    inner, queries, packed = local_pass(
        query_logits,
        value_rows,
        onward_forget_logits,
        reverse_forget_logits,
        onward_floor_gap[None],
        reverse_floor_gap[None],
        extra_log_decay.reshape(1, rows),
    )
    packed, output_matrix, residual = lax.optimization_barrier((packed, output_matrix, residual))
    back = states_around(packed)
    blocks = spread_over_x(output_matrix, residual, inner_norm_gain, inner_norm_bias)
    gated = gated_rows(back, inner, queries, per_head_gain[None], output_gate_logits)
    everyone = lax.all_to_all(gated, ("yb", "x"), 0, 0, tiled=True)
    everyone = lax.all_gather(everyone, "c")
    both = []
    for block in blocks:
        both += [block, lax.ppermute(block, "c", SWAP)]
    middle, own = middle_rows(everyone, both)
    core = lax.axis_index("c").astype(jnp.int32)[None]
    send, hidden = feed_enter(core, middle, weights)
    other = lax.ppermute(send, "c", SWAP)
    mine = feed_leave(core, hidden, weights)
    shares = lax.all_to_all(joined(mine, other), ("yb", "x"), 0, 0, tiled=True)
    before_final, moments = pl.pallas_call(
        total_kernel,
        out_shape=[
            pltpu.VMEM(own.shape, jnp.float32),
            pltpu.VMEM((8, 1, 2 * rows), jnp.float32),
        ],
        compiler_params=pltpu.CompilerParams(vmem_limit_bytes=4 << 20),
        name="total",
    )(*near(shares, own))
    moments = lax.all_to_all(moments, TP, 0, 0, tiled=True)
    return pl.pallas_call(
        closing_kernel,
        out_shape=jax.ShapeDtypeStruct(own.shape, jnp.bfloat16),
        compiler_params=pltpu.CompilerParams(vmem_limit_bytes=4 << 20),
        name="closing",
    )(*near(moments, before_final, closing_norm_gain[None], closing_norm_bias[None]))


def solution(mesh):
    torus = Mesh(mesh.devices.reshape(16, 2, 2, 4, 2), ("z", "ya", "yb", "x", "c"))
    in_specs = (
        P(SP, TP),
        P(SP, TP),
        P(SP, TP),
        P(SP, TP),
        P(SP, TP),
        P(TP),
        P(TP),
        P(SP, TP),
        P(),
        P(SP, TP),
        P(None, TP),
        P(TP),
        P(TP),
        P(SP, TP),
        P(SP, TP),
        P(TP, SP),
        P(TP),
        P(TP),
    )
    out_specs = P(SP, TP)
    return jax.shard_map(layer, mesh=torus, in_specs=in_specs, out_specs=out_specs, check_vma=False)
```

```python
import jax
import jax.numpy as jnp
from jax import lax
from jax.experimental import pallas as pl
from jax.experimental.pallas import tpu as pltpu
from jax.sharding import Mesh
from jax.sharding import PartitionSpec as P


D = 2048
Z = ("zb", "zr")
NEAR = ("zr", "ya", "yb")
SP = ("zb", "zr", "ya", "yb")
TP = ("x", "c")
HALF = 352
SLICE = 16
BLOCK = 8

highest_precision = lax.Precision.HIGHEST
alpha_mix = 2.0**0.25
norm_eps = 1e-05
head_eps = 1e-06


def exact_dot(a, b, dims=((1,), (0,))):
    return lax.dot_general(
        a, b, (dims, ((), ())), precision=highest_precision, preferred_element_type=jnp.float32
    )


def two_terms(x):
    high = x.astype(jnp.bfloat16).astype(jnp.float32)
    return high, (x - high).astype(jnp.bfloat16).astype(jnp.float32)


def local_kernel(
    query_ref,
    value_ref,
    onward_ref,
    reverse_ref,
    onward_gap_ref,
    reverse_gap_ref,
    extra_ref,
    inner_ref,
    queries_ref,
    packed_ref,
    rows_ref,
):
    rows, width = query_ref.shape
    logits = query_ref[...].astype(jnp.float32)
    query = logits / (1.0 + jnp.exp(-logits))
    values = value_ref[...].astype(jnp.float32)
    extra = extra_ref[...]
    at = lax.broadcasted_iota(jnp.int32, (rows, rows), 0)
    source = lax.broadcasted_iota(jnp.int32, (rows, rows), 1)
    ones = jnp.ones((rows, width), jnp.float32)
    inner = jnp.zeros_like(query)
    rows_ref[:, 2 * SLICE :, :] = jnp.zeros((BLOCK, 8, width), jnp.float32)
    for side, (forget_ref, gap_ref, seen, last) in enumerate(
        (
            (onward_ref, onward_gap_ref, at >= source, rows - 1),
            (reverse_ref, reverse_gap_ref, at <= source, 0),
        )
    ):
        seen = seen.astype(jnp.float32)
        keys = gap_ref[...] / (1.0 + jnp.exp(forget_ref[...].astype(jnp.float32)))
        running = exact_dot(seen, jnp.log1p(-keys)) + exact_dot(seen * extra, ones)
        total = running[last : last + 1]
        decayed_query = query * jnp.exp(running)
        scores = exact_dot(decayed_query, keys * jnp.exp(-running), ((1,), (1,))) * seen
        inner = inner + exact_dot(scores, values)
        queries_ref[:, width * side : width * (side + 1)] = decayed_query
        state = exact_dot(values, keys * jnp.exp(total - running), ((0,), (0,)))
        terms = two_terms(total)
        for y in range(BLOCK):
            rows_ref[y, SLICE * side : SLICE * (side + 1), :] = state[
                SLICE * y : SLICE * (y + 1)
            ]
            for t in range(2):
                at_row = 2 * SLICE + 2 * side + t
                rows_ref[y, at_row : at_row + 1, :] = terms[t]
    packed_ref[...] = rows_ref[...].astype(jnp.bfloat16)
    inner_ref[...] = inner


def near(*arrays):
    return [pltpu.with_memory_space_constraint(a, pltpu.VMEM) for a in arrays]


def local_pass(*arrays):
    rows, width = arrays[0].shape
    return pl.pallas_call(
        local_kernel,
        out_shape=[
            pltpu.VMEM((rows, width), jnp.float32),
            pltpu.VMEM((rows, 2 * width), jnp.float32),
            pltpu.VMEM((BLOCK, 2 * SLICE + 8, width), jnp.bfloat16),
        ],
        scratch_shapes=[pltpu.VMEM((BLOCK, 2 * SLICE + 8, width), jnp.float32)],
        compiler_params=pltpu.CompilerParams(vmem_limit_bytes=6 << 20),
        name="local",
    )(*near(*arrays))


def plane_parts(arrived_ref):
    parts = []
    for side in range(2):
        part = []
        for y in range(BLOCK):
            block = arrived_ref[y].astype(jnp.float32)
            decay = block[2 * SLICE + 2 * side : 2 * SLICE + 2 * side + 1]
            decay = decay + block[2 * SLICE + 2 * side + 1 : 2 * SLICE + 2 * side + 2]
            part.append((decay, block[SLICE * side : SLICE * (side + 1)]))
        parts.append(part)
    return parts


def plane_kernel(z_ref, arrived_ref, out_ref, rows_ref):
    forward, backward = plane_parts(arrived_ref)
    wholes = []
    for part in (forward, backward[::-1]):
        decay, state = part[0]
        for next_decay, next_state in part[1:]:
            decay, state = decay + next_decay, jnp.exp(next_decay) * state + next_state
        wholes.append((decay, state))
    for side, (decay, state) in enumerate(wholes):
        rows_ref[side] = jnp.zeros(rows_ref.shape[1:], jnp.float32)
        rows_ref[side, :SLICE, :] = state
        for t, term in enumerate(two_terms(decay)):
            rows_ref[side, SLICE + t : SLICE + t + 1, :] = term
    ahead, behind = rows_ref[0].astype(jnp.bfloat16), rows_ref[1].astype(jnp.bfloat16)
    z = z_ref[0]
    for other in range(out_ref.shape[0]):

        @pl.when(other > z)
        def _():
            out_ref[other] = ahead

        @pl.when(other <= z)
        def _():
            out_ref[other] = behind


def before_kernel(z_ref, planes_ref, arrived_ref, out_ref):
    z = z_ref[0]
    planes = planes_ref.shape[0]
    width = planes_ref.shape[2]
    states = []
    for order in (range(planes), reversed(range(planes))):
        state = jnp.zeros((SLICE, width), jnp.float32)
        for other in order:
            block = planes_ref[other].astype(jnp.float32)
            decay = block[SLICE : SLICE + 1] + block[SLICE + 1 : SLICE + 2]
            passed = other < z if not states else other > z
            state = jnp.where(passed, jnp.exp(decay) * state + block[:SLICE], state)
        states.append(state)
    forward, backward = plane_parts(arrived_ref)
    for side, part in enumerate((forward, backward)):
        state = states[side]
        for y in range(BLOCK) if side == 0 else reversed(range(BLOCK)):
            out_ref[y, SLICE * side : SLICE * (side + 1)] = state.astype(jnp.bfloat16)
            decay, own = part[y]
            state = jnp.exp(decay) * state + own


def states_around(packed):
    z = lax.axis_index("zb").astype(jnp.int32)[None]
    planes = lax.axis_size("zb")
    width = packed.shape[2]
    (arrived,) = near(lax.all_to_all(packed, NEAR, 0, 0, tiled=True))
    totals = pl.pallas_call(
        plane_kernel,
        in_specs=[SMEM, VMEM],
        out_specs=VMEM,
        out_shape=pltpu.VMEM((planes, SLICE + 8, width), jnp.bfloat16),
        scratch_shapes=[pltpu.VMEM((2, SLICE + 8, width), jnp.float32)],
        compiler_params=pltpu.CompilerParams(vmem_limit_bytes=4 << 20),
        name="plane",
    )(z, arrived)
    (others,) = near(lax.all_to_all(totals, "zb", 0, 0, tiled=True))
    before = pl.pallas_call(
        before_kernel,
        in_specs=[SMEM, VMEM, VMEM],
        out_specs=VMEM,
        out_shape=pltpu.VMEM((BLOCK, 2 * SLICE, width), jnp.bfloat16),
        compiler_params=pltpu.CompilerParams(vmem_limit_bytes=4 << 20),
        name="before",
    )(z, others, arrived)
    return lax.all_to_all(before, NEAR, 0, 0, tiled=True)


def gated_kernel(back_ref, inner_ref, queries_ref, gain_ref, gate_ref, out_ref):
    width = inner_ref.shape[1]
    mixed = inner_ref[...]
    for side in range(2):
        state = [back_ref[y, SLICE * side : SLICE * (side + 1)] for y in range(BLOCK)]
        state = jnp.concatenate([part.astype(jnp.float32) for part in state], axis=0)
        queries = queries_ref[:, width * side : width * (side + 1)]
        mixed = mixed + exact_dot(queries, state, ((1,), (1,)))
    mean = jnp.mean(mixed * mixed, axis=1, keepdims=True)
    normed = mixed * lax.rsqrt(mean + head_eps) * gain_ref[...]
    gate = gate_ref[...].astype(jnp.float32)
    gated = (normed * (gate / (1.0 + jnp.exp(-gate)))).astype(jnp.bfloat16)
    for peer in range(out_ref.shape[0]):
        out_ref[peer] = gated


def gated_rows(*arrays):
    return pl.pallas_call(
        gated_kernel,
        out_shape=pltpu.VMEM((8, *arrays[1].shape), jnp.bfloat16),
        compiler_params=pltpu.CompilerParams(vmem_limit_bytes=4 << 20),
        name="gated",
    )(*near(*arrays))


SMEM = pl.BlockSpec(memory_space=pltpu.SMEM)
VMEM = pl.BlockSpec(memory_space=pltpu.VMEM)
ANY = pl.BlockSpec(memory_space=pl.ANY)


def turn_kernel(in_ref, out_ref):
    for kind in range(3):
        rows = jnp.concatenate([in_ref[y, kind] for y in range(4)], axis=0)
        out_ref[kind] = rows.T


def gathered_weights(gate, up, down):
    both = jnp.stack([gate, up, down.T])
    halves = [both[:, :, :HALF], both[:, :, HALF:]]
    arrived = lax.all_to_all(jnp.stack(halves + halves), ("ya", "yb"), 0, 0, tiled=True)
    shard = pl.pallas_call(
        turn_kernel,
        out_shape=jax.ShapeDtypeStruct((3, HALF, 128), jnp.bfloat16),
        compiler_params=pltpu.CompilerParams(vmem_limit_bytes=6 << 20),
        name="turn",
    )(*near(arrived)).reshape(3 * HALF, 128)
    weights = lax.all_gather(shard, Z, axis=0, tiled=True).reshape(-1, 3, HALF, 128)
    return pltpu.with_memory_space_constraint(weights, pltpu.HBM)


def exact_terms(x):
    terms = []
    for _ in range(3):
        term = lax.reduce_precision(x, 8, 7)
        terms.append(term.astype(jnp.bfloat16))
        x = x - term
    return terms


SWAP = ((0, 1), (1, 0))


def spread_over_x(output_matrix, residual, gain, bias):
    other = lax.ppermute(residual, "yb", SWAP)
    first = lax.axis_index("yb") == 0
    vectors = jnp.stack(exact_terms(gain) + exact_terms(bias))
    block = jnp.concatenate(
        [
            output_matrix,
            jnp.where(first, residual, other),
            jnp.where(first, other, residual),
            jnp.pad(vectors, ((0, 10), (0, 0))),
        ]
    )
    count = lax.axis_size("x")
    return [block] + [
        lax.ppermute(block, "x", [(i, (i + k) % count) for i in range(count)])
        for k in range(1, count)
    ]


def middle_kernel(place_ref, gated_ref, *refs):
    block_refs, (out_ref, own_ref, whole_ref, before_ref) = refs[:8], refs[8:]
    heads, rows = 8, gated_ref.shape[2]
    count = 2 * rows
    for core in range(2):
        for pair in range(2):
            for x in range(4):
                head = 2 * x + core
                whole_ref[pair * rows : (pair + 1) * rows, 128 * head : 128 * head + 128] = (
                    gated_ref[core, 4 * pair + x]
                )
    whole = whole_ref[...]
    inner = whole.shape[1]
    total = jnp.zeros((count, 1), jnp.float32)
    for b in range(heads):
        mixer = jnp.dot(whole, block_refs[b][:inner], preferred_element_type=jnp.float32)
        residual = block_refs[b][inner : inner + count].astype(jnp.float32)
        before = alpha_mix * residual + mixer
        before_ref[b] = before
        total = total + jnp.sum(before, axis=1, keepdims=True)
    mean = total / D
    spread = jnp.zeros((count, 1), jnp.float32)
    for b in range(heads):
        centre = before_ref[b] - mean
        spread = spread + jnp.sum(centre * centre, axis=1, keepdims=True)
    scale = lax.rsqrt(spread / D + norm_eps)
    for b in range(heads):
        vectors = block_refs[b][inner + count : inner + count + 16].astype(jnp.float32)
        gain = vectors[0:1] + vectors[1:2] + vectors[2:3]
        bias = vectors[3:4] + vectors[4:5] + vectors[5:6]
        normed = (before_ref[b] - mean) * scale * gain + bias
        normed = normed.astype(jnp.bfloat16)
        out_ref[place_ref[b]] = normed
        if b == 0:
            own_ref[...] = jnp.where(place_ref[heads] == 0, normed[:rows], normed[rows:])


def middle_rows(gated, blocks):
    rows, width = gated.shape[2], blocks[0].shape[1]
    x, core = lax.axis_index("x"), lax.axis_index("c")
    place = [2 * ((x - b // 2 + 4) % 4) + (core + b) % 2 for b in range(8)]
    place = jnp.stack(place + [lax.axis_index("yb")])
    vmem = pl.BlockSpec(memory_space=pltpu.VMEM)
    return pl.pallas_call(
        middle_kernel,
        in_specs=[pl.BlockSpec(memory_space=pltpu.SMEM)] + [vmem] * 9,
        out_specs=[vmem, vmem],
        out_shape=[
            pltpu.VMEM((8, 2 * rows, width), jnp.bfloat16),
            pltpu.VMEM((rows, width), jnp.bfloat16),
        ],
        scratch_shapes=[
            pltpu.VMEM((2 * rows, 8 * 128), jnp.bfloat16),
            pltpu.VMEM((8, 2 * rows, width), jnp.float32),
        ],
        compiler_params=pltpu.CompilerParams(vmem_limit_bytes=14 << 20),
        name="middle",
    )(place.astype(jnp.int32), *near(gated), *blocks)


def leaving(hidden, down_ref, block):
    wide = jnp.concatenate([down_ref[2 * block], down_ref[2 * block + 1]], axis=1)
    return jnp.dot(hidden, wide, preferred_element_type=jnp.float32)


def down_copies(core, weights_ref, leave_ref, sem_ref):
    copies = []
    for s in range(4):
        copies.append(
            pltpu.make_async_copy(
                weights_ref.at[pl.ds(4 * s + 2 * core, 2), 2],
                leave_ref.at[pl.ds(2 * s, 2)],
                sem_ref.at[s],
            )
        )
    return copies


def enter_kernel(
    core_ref, rows_ref, weights_ref, send_ref, hidden_ref, enter_ref, leave_ref, enter_sem, leave_sem
):
    parts, each = 4, 4
    copies = []
    for s in range(parts):
        copies.append(
            pltpu.make_async_copy(
                weights_ref.at[pl.ds(s * each, each), pl.ds(0, 2)],
                enter_ref.at[pl.ds(s * each, each)],
                enter_sem.at[s],
            )
        )
    downs = down_copies(1 - core_ref[0], weights_ref, leave_ref, leave_sem)
    for copy in copies + downs:
        copy.start()
    sums = [0.0, 0.0]
    for s in range(parts):
        x = jnp.concatenate([rows_ref[2 * s], rows_ref[2 * s + 1]], axis=1)
        copies[s].wait()
        for kind in range(2):
            wide = [enter_ref[each * s + j, kind] for j in range(each)]
            sums[kind] += lax.dot_general(
                x,
                jnp.concatenate(wide, axis=1),
                (((1,), (1,)), ((), ())),
                preferred_element_type=jnp.float32,
            )
    gate, up = sums
    hidden = (gate / (1.0 + jnp.exp(-gate)) * up).astype(jnp.bfloat16)
    hidden_ref[...] = hidden
    rows = send_ref.shape[2]
    for s in range(4):
        downs[s].wait()
        product = leaving(hidden, leave_ref, s).astype(jnp.bfloat16)
        send_ref[0, s] = product[:rows]
        send_ref[1, s] = product[rows:]


def leave_kernel(core_ref, hidden_ref, weights_ref, out_ref, leave_ref, leave_sem):
    downs = down_copies(core_ref[0], weights_ref, leave_ref, leave_sem)
    for copy in downs:
        copy.start()
    hidden = hidden_ref[...]
    rows = out_ref.shape[2]
    for s in range(4):
        downs[s].wait()
        product = leaving(hidden, leave_ref, s)
        out_ref[0, s] = product[:rows]
        out_ref[1, s] = product[rows:]


def join_kernel(mine_ref, other_ref, out_ref):
    for pair in range(2):
        for s in range(4):
            total = mine_ref[pair, s] + other_ref[pair, s].astype(jnp.float32)
            out_ref[2 * s + pair] = total.astype(jnp.bfloat16)


def feed_enter(core, rows, weights):
    blocks, count, width = rows.shape
    return pl.pallas_call(
        enter_kernel,
        in_specs=[SMEM, VMEM, ANY],
        out_specs=[VMEM, VMEM],
        out_shape=[
            pltpu.VMEM((2, blocks // 2, count // 2, width), jnp.bfloat16),
            pltpu.VMEM((count, HALF), jnp.bfloat16),
        ],
        scratch_shapes=[
            pltpu.VMEM((16, 2, HALF, 128), jnp.bfloat16),
            pltpu.VMEM((8, HALF, 128), jnp.bfloat16),
            pltpu.SemaphoreType.DMA((4,)),
            pltpu.SemaphoreType.DMA((4,)),
        ],
        cost_estimate=pl.CostEstimate(
            flops=5 * count * D * HALF, bytes_accessed=5 * D * HALF, transcendentals=count * HALF
        ),
        compiler_params=pltpu.CompilerParams(vmem_limit_bytes=16 << 20),
        name="feed_enter",
    )(core, *near(rows), weights)


def feed_leave(core, hidden, weights):
    count = hidden.shape[0]
    return pl.pallas_call(
        leave_kernel,
        in_specs=[SMEM, VMEM, ANY],
        out_specs=VMEM,
        out_shape=pltpu.VMEM((2, 4, count // 2, 256), jnp.float32),
        scratch_shapes=[
            pltpu.VMEM((8, HALF, 128), jnp.bfloat16),
            pltpu.SemaphoreType.DMA((4,)),
        ],
        cost_estimate=pl.CostEstimate(
            flops=count * D * HALF, bytes_accessed=D * HALF, transcendentals=0
        ),
        compiler_params=pltpu.CompilerParams(vmem_limit_bytes=8 << 20),
        name="feed_leave",
    )(core, *near(hidden), weights)


def joined(mine, other):
    return pl.pallas_call(
        join_kernel,
        out_shape=pltpu.VMEM((8, *mine.shape[2:]), jnp.bfloat16),
        compiler_params=pltpu.CompilerParams(vmem_limit_bytes=8 << 20),
        name="join",
    )(*near(mine, other))


def diagonal_of(rows):
    at = lax.broadcasted_iota(jnp.int32, (rows, rows), 0)
    return (at == lax.broadcasted_iota(jnp.int32, (rows, rows), 1)).astype(jnp.float32)


def total_kernel(arrived_ref, own_ref, before_ref, moments_ref):
    feed = arrived_ref[0].astype(jnp.float32)
    for peer in range(1, arrived_ref.shape[0]):
        feed = feed + arrived_ref[peer].astype(jnp.float32)
    before = alpha_mix * own_ref[...].astype(jnp.float32) + feed
    before_ref[...] = before
    diagonal = diagonal_of(before.shape[0])
    moments = []
    for value in (before, before * before):
        column = jnp.sum(value, axis=1, keepdims=True)
        moments.append(jnp.sum(diagonal * column, axis=0, keepdims=True))
    moments = jnp.concatenate(moments, axis=1)
    for peer in range(moments_ref.shape[0]):
        moments_ref[peer] = moments


def closing_kernel(moments_ref, before_ref, gain_ref, bias_ref, out_ref):
    moments = moments_ref[0]
    for peer in range(1, moments_ref.shape[0]):
        moments = moments + moments_ref[peer]
    rows = before_ref.shape[0]
    mean = moments[:, :rows] / D
    spread = moments[:, rows:] / D - mean * mean
    diagonal = diagonal_of(rows)
    column = jnp.sum(diagonal * mean, axis=1, keepdims=True)
    factor = jnp.sum(diagonal * lax.rsqrt(spread + norm_eps), axis=1, keepdims=True)
    out_ref[...] = ((before_ref[...] - column) * factor * gain_ref[...] + bias_ref[...]).astype(
        jnp.bfloat16
    )


def layer(
    query_logits,
    value_rows,
    onward_forget_logits,
    reverse_forget_logits,
    output_gate_logits,
    onward_floor_gap,
    reverse_floor_gap,
    extra_log_decay,
    per_head_gain,
    residual,
    output_matrix,
    inner_norm_gain,
    inner_norm_bias,
    gate_matrix,
    up_matrix,
    down_matrix,
    closing_norm_gain,
    closing_norm_bias,
):
    weights = gathered_weights(gate_matrix, up_matrix, down_matrix)
    rows = query_logits.shape[0]
    inner, queries, packed = local_pass(
        query_logits,
        value_rows,
        onward_forget_logits,
        reverse_forget_logits,
        onward_floor_gap[None],
        reverse_floor_gap[None],
        extra_log_decay.reshape(1, rows),
    )
    packed, output_matrix, residual = lax.optimization_barrier((packed, output_matrix, residual))
    back = states_around(packed)
    blocks = spread_over_x(output_matrix, residual, inner_norm_gain, inner_norm_bias)
    gated = gated_rows(back, inner, queries, per_head_gain[None], output_gate_logits)
    everyone = lax.all_to_all(gated, ("yb", "x"), 0, 0, tiled=True)
    everyone = lax.all_gather(everyone, "c")
    both = []
    for block in blocks:
        both += [block, lax.ppermute(block, "c", SWAP)]
    middle, own = middle_rows(everyone, both)
    core = lax.axis_index("c").astype(jnp.int32)[None]
    send, hidden = feed_enter(core, middle, weights)
    other = lax.ppermute(send, "c", SWAP)
    mine = feed_leave(core, hidden, weights)
    shares = lax.all_to_all(joined(mine, other), ("x", "yb"), 0, 0, tiled=True)
    before_final, moments = pl.pallas_call(
        total_kernel,
        out_shape=[
            pltpu.VMEM(own.shape, jnp.float32),
            pltpu.VMEM((8, 1, 2 * rows), jnp.float32),
        ],
        compiler_params=pltpu.CompilerParams(vmem_limit_bytes=4 << 20),
        name="total",
    )(*near(shares, own))
    moments = lax.all_to_all(moments, TP, 0, 0, tiled=True)
    return pl.pallas_call(
        closing_kernel,
        out_shape=jax.ShapeDtypeStruct(own.shape, jnp.bfloat16),
        compiler_params=pltpu.CompilerParams(vmem_limit_bytes=4 << 20),
        name="closing",
    )(*near(moments, before_final, closing_norm_gain[None], closing_norm_bias[None]))


def solution(mesh):
    torus = Mesh(mesh.devices.reshape(8, 2, 2, 2, 4, 2), ("zb", "zr", "ya", "yb", "x", "c"))
    in_specs = (
        P(SP, TP),
        P(SP, TP),
        P(SP, TP),
        P(SP, TP),
        P(SP, TP),
        P(TP),
        P(TP),
        P(SP, TP),
        P(),
        P(SP, TP),
        P(None, TP),
        P(TP),
        P(TP),
        P(SP, TP),
        P(SP, TP),
        P(TP, SP),
        P(TP),
        P(TP),
    )
    out_specs = P(SP, TP)
    return jax.shard_map(layer, mesh=torus, in_specs=in_specs, out_specs=out_specs, check_vma=False)
```

```python
import jax
import jax.numpy as jnp
from jax import lax
from jax.experimental import pallas as pl
from jax.experimental.pallas import tpu as pltpu
from jax.sharding import Mesh
from jax.sharding import PartitionSpec as P


D = 2048
Z = ("zb", "zr")
NEAR = ("zr", "ya", "yb")
SP = ("zb", "zr", "ya", "yb")
TP = ("x", "c")
HALF = 352
SLICE = 16
BLOCK = 8

highest_precision = lax.Precision.HIGHEST
alpha_mix = 2.0**0.25
norm_eps = 1e-05
head_eps = 1e-06


def exact_dot(a, b, dims=((1,), (0,))):
    return lax.dot_general(
        a, b, (dims, ((), ())), precision=highest_precision, preferred_element_type=jnp.float32
    )


def two_terms(x):
    high = x.astype(jnp.bfloat16).astype(jnp.float32)
    return high, (x - high).astype(jnp.bfloat16).astype(jnp.float32)


def local_kernel(
    query_ref,
    value_ref,
    onward_ref,
    reverse_ref,
    onward_gap_ref,
    reverse_gap_ref,
    extra_ref,
    inner_ref,
    queries_ref,
    packed_ref,
    rows_ref,
):
    rows, width = query_ref.shape
    logits = query_ref[...].astype(jnp.float32)
    query = logits / (1.0 + jnp.exp(-logits))
    values = value_ref[...].astype(jnp.float32)
    extra = extra_ref[...]
    at = lax.broadcasted_iota(jnp.int32, (rows, rows), 0)
    source = lax.broadcasted_iota(jnp.int32, (rows, rows), 1)
    ones = jnp.ones((rows, width), jnp.float32)
    inner = jnp.zeros_like(query)
    rows_ref[:, 2 * SLICE :, :] = jnp.zeros((BLOCK, 8, width), jnp.float32)
    for side, (forget_ref, gap_ref, seen, last) in enumerate(
        (
            (onward_ref, onward_gap_ref, at >= source, rows - 1),
            (reverse_ref, reverse_gap_ref, at <= source, 0),
        )
    ):
        seen = seen.astype(jnp.float32)
        keys = gap_ref[...] / (1.0 + jnp.exp(forget_ref[...].astype(jnp.float32)))
        running = exact_dot(seen, jnp.log1p(-keys)) + exact_dot(seen * extra, ones)
        total = running[last : last + 1]
        decayed_query = query * jnp.exp(running)
        scores = exact_dot(decayed_query, keys * jnp.exp(-running), ((1,), (1,))) * seen
        inner = inner + exact_dot(scores, values)
        queries_ref[:, width * side : width * (side + 1)] = decayed_query
        state = exact_dot(values, keys * jnp.exp(total - running), ((0,), (0,)))
        terms = two_terms(total)
        for y in range(BLOCK):
            rows_ref[y, SLICE * side : SLICE * (side + 1), :] = state[
                SLICE * y : SLICE * (y + 1)
            ]
            for t in range(2):
                at_row = 2 * SLICE + 2 * side + t
                rows_ref[y, at_row : at_row + 1, :] = terms[t]
    packed_ref[...] = rows_ref[...].astype(jnp.bfloat16)
    inner_ref[...] = inner


def near(*arrays):
    return [pltpu.with_memory_space_constraint(a, pltpu.VMEM) for a in arrays]


def local_pass(*arrays):
    rows, width = arrays[0].shape
    return pl.pallas_call(
        local_kernel,
        out_shape=[
            pltpu.VMEM((rows, width), jnp.float32),
            pltpu.VMEM((rows, 2 * width), jnp.float32),
            pltpu.VMEM((BLOCK, 2 * SLICE + 8, width), jnp.bfloat16),
        ],
        scratch_shapes=[pltpu.VMEM((BLOCK, 2 * SLICE + 8, width), jnp.float32)],
        compiler_params=pltpu.CompilerParams(vmem_limit_bytes=6 << 20),
        name="local",
    )(*near(*arrays))


def plane_parts(arrived_ref):
    parts = []
    for side in range(2):
        part = []
        for y in range(BLOCK):
            block = arrived_ref[y].astype(jnp.float32)
            decay = block[2 * SLICE + 2 * side : 2 * SLICE + 2 * side + 1]
            decay = decay + block[2 * SLICE + 2 * side + 1 : 2 * SLICE + 2 * side + 2]
            part.append((decay, block[SLICE * side : SLICE * (side + 1)]))
        parts.append(part)
    return parts


def plane_kernel(z_ref, arrived_ref, out_ref, rows_ref):
    forward, backward = plane_parts(arrived_ref)
    wholes = []
    for part in (forward, backward[::-1]):
        decay, state = part[0]
        for next_decay, next_state in part[1:]:
            decay, state = decay + next_decay, jnp.exp(next_decay) * state + next_state
        wholes.append((decay, state))
    for side, (decay, state) in enumerate(wholes):
        rows_ref[side] = jnp.zeros(rows_ref.shape[1:], jnp.float32)
        rows_ref[side, :SLICE, :] = state
        for t, term in enumerate(two_terms(decay)):
            rows_ref[side, SLICE + t : SLICE + t + 1, :] = term
    ahead, behind = rows_ref[0].astype(jnp.bfloat16), rows_ref[1].astype(jnp.bfloat16)
    z = z_ref[0]
    for other in range(out_ref.shape[0]):

        @pl.when(other > z)
        def _():
            out_ref[other] = ahead

        @pl.when(other <= z)
        def _():
            out_ref[other] = behind


def before_kernel(z_ref, planes_ref, arrived_ref, out_ref):
    z = z_ref[0]
    planes = planes_ref.shape[0]
    width = planes_ref.shape[2]
    states = []
    for order in (range(planes), reversed(range(planes))):
        state = jnp.zeros((SLICE, width), jnp.float32)
        for other in order:
            block = planes_ref[other].astype(jnp.float32)
            decay = block[SLICE : SLICE + 1] + block[SLICE + 1 : SLICE + 2]
            passed = other < z if not states else other > z
            state = jnp.where(passed, jnp.exp(decay) * state + block[:SLICE], state)
        states.append(state)
    forward, backward = plane_parts(arrived_ref)
    for side, part in enumerate((forward, backward)):
        state = states[side]
        for y in range(BLOCK) if side == 0 else reversed(range(BLOCK)):
            out_ref[y, SLICE * side : SLICE * (side + 1)] = state.astype(jnp.bfloat16)
            decay, own = part[y]
            state = jnp.exp(decay) * state + own


def states_around(packed):
    z = lax.axis_index("zb").astype(jnp.int32)[None]
    planes = lax.axis_size("zb")
    width = packed.shape[2]
    (arrived,) = near(lax.all_to_all(packed, NEAR, 0, 0, tiled=True))
    totals = pl.pallas_call(
        plane_kernel,
        in_specs=[SMEM, VMEM],
        out_specs=VMEM,
        out_shape=pltpu.VMEM((planes, SLICE + 8, width), jnp.bfloat16),
        scratch_shapes=[pltpu.VMEM((2, SLICE + 8, width), jnp.float32)],
        compiler_params=pltpu.CompilerParams(vmem_limit_bytes=4 << 20),
        name="plane",
    )(z, arrived)
    (others,) = near(lax.all_to_all(totals, "zb", 0, 0, tiled=True))
    before = pl.pallas_call(
        before_kernel,
        in_specs=[SMEM, VMEM, VMEM],
        out_specs=VMEM,
        out_shape=pltpu.VMEM((BLOCK, 2 * SLICE, width), jnp.bfloat16),
        compiler_params=pltpu.CompilerParams(vmem_limit_bytes=4 << 20),
        name="before",
    )(z, others, arrived)
    return lax.all_to_all(before, NEAR, 0, 0, tiled=True)


def gated_kernel(back_ref, inner_ref, queries_ref, gain_ref, gate_ref, out_ref):
    width = inner_ref.shape[1]
    mixed = inner_ref[...]
    for side in range(2):
        state = [back_ref[y, SLICE * side : SLICE * (side + 1)] for y in range(BLOCK)]
        state = jnp.concatenate([part.astype(jnp.float32) for part in state], axis=0)
        queries = queries_ref[:, width * side : width * (side + 1)]
        mixed = mixed + exact_dot(queries, state, ((1,), (1,)))
    mean = jnp.mean(mixed * mixed, axis=1, keepdims=True)
    normed = mixed * lax.rsqrt(mean + head_eps) * gain_ref[...]
    gate = gate_ref[...].astype(jnp.float32)
    gated = (normed * (gate / (1.0 + jnp.exp(-gate)))).astype(jnp.bfloat16)
    for peer in range(out_ref.shape[0]):
        out_ref[peer] = gated


def gated_rows(*arrays):
    return pl.pallas_call(
        gated_kernel,
        out_shape=pltpu.VMEM((8, *arrays[1].shape), jnp.bfloat16),
        compiler_params=pltpu.CompilerParams(vmem_limit_bytes=4 << 20),
        name="gated",
    )(*near(*arrays))


SMEM = pl.BlockSpec(memory_space=pltpu.SMEM)
VMEM = pl.BlockSpec(memory_space=pltpu.VMEM)
ANY = pl.BlockSpec(memory_space=pl.ANY)


def turn_kernel(in_ref, out_ref, turned_ref, sem_ref):
    copies = []
    for kind in range(3):
        rows = jnp.concatenate([in_ref[y, kind] for y in range(4)], axis=0)
        turned_ref[kind] = rows.T
        copies.append(
            pltpu.make_async_copy(turned_ref.at[kind], out_ref.at[kind], sem_ref.at[kind])
        )
        copies[kind].start()
    for copy in copies:
        copy.wait()


def gathered_weights(gate, up, down):
    both = jnp.stack([gate, up, down.T])
    halves = [both[:, :, :HALF], both[:, :, HALF:]]
    arrived = lax.all_to_all(jnp.stack(halves + halves), ("ya", "yb"), 0, 0, tiled=True)
    shard = pl.pallas_call(
        turn_kernel,
        out_shape=jax.ShapeDtypeStruct((3, HALF, 128), jnp.bfloat16),
        in_specs=[VMEM],
        out_specs=ANY,
        scratch_shapes=[
            pltpu.VMEM((3, HALF, 128), jnp.bfloat16),
            pltpu.SemaphoreType.DMA((3,)),
        ],
        compiler_params=pltpu.CompilerParams(vmem_limit_bytes=6 << 20),
        name="turn",
    )(*near(arrived)).reshape(3 * HALF, 128)
    weights = lax.all_gather(shard, Z, axis=0, tiled=True).reshape(-1, 3, HALF, 128)
    return pltpu.with_memory_space_constraint(weights, pltpu.HBM)


def exact_terms(x):
    terms = []
    for _ in range(3):
        term = lax.reduce_precision(x, 8, 7)
        terms.append(term.astype(jnp.bfloat16))
        x = x - term
    return terms


SWAP = ((0, 1), (1, 0))


def spread_over_x(output_matrix, residual, gain, bias):
    other = lax.ppermute(residual, "yb", SWAP)
    first = lax.axis_index("yb") == 0
    vectors = jnp.stack(exact_terms(gain) + exact_terms(bias))
    block = jnp.concatenate(
        [
            output_matrix,
            jnp.where(first, residual, other),
            jnp.where(first, other, residual),
            jnp.pad(vectors, ((0, 10), (0, 0))),
        ]
    )
    count = lax.axis_size("x")
    return [block] + [
        lax.ppermute(block, "x", [(i, (i + k) % count) for i in range(count)])
        for k in range(1, count)
    ]


def middle_kernel(place_ref, gated_ref, *refs):
    block_refs, (out_ref, own_ref, whole_ref, before_ref) = refs[:8], refs[8:]
    heads, rows = 8, gated_ref.shape[2]
    count = 2 * rows
    for core in range(2):
        for pair in range(2):
            for x in range(4):
                head = 2 * x + core
                whole_ref[pair * rows : (pair + 1) * rows, 128 * head : 128 * head + 128] = (
                    gated_ref[core, 4 * pair + x]
                )
    whole = whole_ref[...]
    inner = whole.shape[1]
    total = jnp.zeros((count, 1), jnp.float32)
    for b in range(heads):
        mixer = jnp.dot(whole, block_refs[b][:inner], preferred_element_type=jnp.float32)
        residual = block_refs[b][inner : inner + count].astype(jnp.float32)
        before = alpha_mix * residual + mixer
        before_ref[b] = before
        total = total + jnp.sum(before, axis=1, keepdims=True)
    mean = total / D
    spread = jnp.zeros((count, 1), jnp.float32)
    for b in range(heads):
        centre = before_ref[b] - mean
        spread = spread + jnp.sum(centre * centre, axis=1, keepdims=True)
    scale = lax.rsqrt(spread / D + norm_eps)
    for b in range(heads):
        vectors = block_refs[b][inner + count : inner + count + 16].astype(jnp.float32)
        gain = vectors[0:1] + vectors[1:2] + vectors[2:3]
        bias = vectors[3:4] + vectors[4:5] + vectors[5:6]
        normed = (before_ref[b] - mean) * scale * gain + bias
        normed = normed.astype(jnp.bfloat16)
        out_ref[place_ref[b]] = normed
        if b == 0:
            own_ref[...] = jnp.where(place_ref[heads] == 0, normed[:rows], normed[rows:])


def middle_rows(gated, blocks):
    rows, width = gated.shape[2], blocks[0].shape[1]
    x, core = lax.axis_index("x"), lax.axis_index("c")
    place = [2 * ((x - b // 2 + 4) % 4) + (core + b) % 2 for b in range(8)]
    place = jnp.stack(place + [lax.axis_index("yb")])
    vmem = pl.BlockSpec(memory_space=pltpu.VMEM)
    return pl.pallas_call(
        middle_kernel,
        in_specs=[pl.BlockSpec(memory_space=pltpu.SMEM)] + [vmem] * 9,
        out_specs=[vmem, vmem],
        out_shape=[
            pltpu.VMEM((8, 2 * rows, width), jnp.bfloat16),
            pltpu.VMEM((rows, width), jnp.bfloat16),
        ],
        scratch_shapes=[
            pltpu.VMEM((2 * rows, 8 * 128), jnp.bfloat16),
            pltpu.VMEM((8, 2 * rows, width), jnp.float32),
        ],
        compiler_params=pltpu.CompilerParams(vmem_limit_bytes=14 << 20),
        name="middle",
    )(place.astype(jnp.int32), *near(gated), *blocks)


def leaving(hidden, down_ref, block):
    wide = jnp.concatenate([down_ref[2 * block], down_ref[2 * block + 1]], axis=1)
    return jnp.dot(hidden, wide, preferred_element_type=jnp.float32)


def down_copies(core, weights_ref, leave_ref, sem_ref):
    copies = []
    for s in range(4):
        copies.append(
            pltpu.make_async_copy(
                weights_ref.at[pl.ds(4 * s + 2 * core, 2), 2],
                leave_ref.at[pl.ds(2 * s, 2)],
                sem_ref.at[s],
            )
        )
    return copies


def enter_kernel(
    core_ref, rows_ref, weights_ref, send_ref, hidden_ref, enter_ref, leave_ref, enter_sem, leave_sem
):
    parts, each = 4, 4
    copies = []
    for s in range(parts):
        copies.append(
            pltpu.make_async_copy(
                weights_ref.at[pl.ds(s * each, each), pl.ds(0, 2)],
                enter_ref.at[pl.ds(s * each, each)],
                enter_sem.at[s],
            )
        )
    downs = down_copies(1 - core_ref[0], weights_ref, leave_ref, leave_sem)
    for copy in copies + downs:
        copy.start()
    sums = [0.0, 0.0]
    for s in range(parts):
        x = jnp.concatenate([rows_ref[2 * s], rows_ref[2 * s + 1]], axis=1)
        copies[s].wait()
        for kind in range(2):
            wide = [enter_ref[each * s + j, kind] for j in range(each)]
            sums[kind] += lax.dot_general(
                x,
                jnp.concatenate(wide, axis=1),
                (((1,), (1,)), ((), ())),
                preferred_element_type=jnp.float32,
            )
    gate, up = sums
    hidden = (gate / (1.0 + jnp.exp(-gate)) * up).astype(jnp.bfloat16)
    hidden_ref[...] = hidden
    rows = send_ref.shape[2]
    for s in range(4):
        downs[s].wait()
        product = leaving(hidden, leave_ref, s).astype(jnp.bfloat16)
        send_ref[0, s] = product[:rows]
        send_ref[1, s] = product[rows:]


def leave_kernel(core_ref, hidden_ref, weights_ref, out_ref, leave_ref, leave_sem):
    downs = down_copies(core_ref[0], weights_ref, leave_ref, leave_sem)
    for copy in downs:
        copy.start()
    hidden = hidden_ref[...]
    rows = out_ref.shape[2]
    for s in range(4):
        downs[s].wait()
        product = leaving(hidden, leave_ref, s)
        out_ref[0, s] = product[:rows]
        out_ref[1, s] = product[rows:]


def join_kernel(mine_ref, other_ref, out_ref):
    for pair in range(2):
        for s in range(4):
            total = mine_ref[pair, s] + other_ref[pair, s].astype(jnp.float32)
            out_ref[4 * pair + s] = total.astype(jnp.bfloat16)


def feed_enter(core, rows, weights):
    blocks, count, width = rows.shape
    return pl.pallas_call(
        enter_kernel,
        in_specs=[SMEM, VMEM, ANY],
        out_specs=[VMEM, VMEM],
        out_shape=[
            pltpu.VMEM((2, blocks // 2, count // 2, width), jnp.bfloat16),
            pltpu.VMEM((count, HALF), jnp.bfloat16),
        ],
        scratch_shapes=[
            pltpu.VMEM((16, 2, HALF, 128), jnp.bfloat16),
            pltpu.VMEM((8, HALF, 128), jnp.bfloat16),
            pltpu.SemaphoreType.DMA((4,)),
            pltpu.SemaphoreType.DMA((4,)),
        ],
        cost_estimate=pl.CostEstimate(
            flops=5 * count * D * HALF, bytes_accessed=5 * D * HALF, transcendentals=count * HALF
        ),
        compiler_params=pltpu.CompilerParams(vmem_limit_bytes=16 << 20),
        name="feed_enter",
    )(core, *near(rows), weights)


def feed_leave(core, hidden, weights):
    count = hidden.shape[0]
    return pl.pallas_call(
        leave_kernel,
        in_specs=[SMEM, VMEM, ANY],
        out_specs=VMEM,
        out_shape=pltpu.VMEM((2, 4, count // 2, 256), jnp.float32),
        scratch_shapes=[
            pltpu.VMEM((8, HALF, 128), jnp.bfloat16),
            pltpu.SemaphoreType.DMA((4,)),
        ],
        cost_estimate=pl.CostEstimate(
            flops=count * D * HALF, bytes_accessed=D * HALF, transcendentals=0
        ),
        compiler_params=pltpu.CompilerParams(vmem_limit_bytes=8 << 20),
        name="feed_leave",
    )(core, *near(hidden), weights)


def joined(mine, other):
    return pl.pallas_call(
        join_kernel,
        out_shape=pltpu.VMEM((8, *mine.shape[2:]), jnp.bfloat16),
        compiler_params=pltpu.CompilerParams(vmem_limit_bytes=8 << 20),
        name="join",
    )(*near(mine, other))


def diagonal_of(rows):
    at = lax.broadcasted_iota(jnp.int32, (rows, rows), 0)
    return (at == lax.broadcasted_iota(jnp.int32, (rows, rows), 1)).astype(jnp.float32)


def total_kernel(arrived_ref, own_ref, before_ref, moments_ref):
    feed = arrived_ref[0].astype(jnp.float32)
    for peer in range(1, arrived_ref.shape[0]):
        feed = feed + arrived_ref[peer].astype(jnp.float32)
    before = alpha_mix * own_ref[...].astype(jnp.float32) + feed
    before_ref[...] = before
    diagonal = diagonal_of(before.shape[0])
    moments = []
    for value in (before, before * before):
        column = jnp.sum(value, axis=1, keepdims=True)
        moments.append(jnp.sum(diagonal * column, axis=0, keepdims=True))
    moments = jnp.concatenate(moments, axis=1)
    for peer in range(moments_ref.shape[0]):
        moments_ref[peer] = moments


def closing_kernel(moments_ref, before_ref, gain_ref, bias_ref, out_ref):
    moments = moments_ref[0]
    for peer in range(1, moments_ref.shape[0]):
        moments = moments + moments_ref[peer]
    rows = before_ref.shape[0]
    mean = moments[:, :rows] / D
    spread = moments[:, rows:] / D - mean * mean
    diagonal = diagonal_of(rows)
    column = jnp.sum(diagonal * mean, axis=1, keepdims=True)
    factor = jnp.sum(diagonal * lax.rsqrt(spread + norm_eps), axis=1, keepdims=True)
    out_ref[...] = ((before_ref[...] - column) * factor * gain_ref[...] + bias_ref[...]).astype(
        jnp.bfloat16
    )


def layer(
    query_logits,
    value_rows,
    onward_forget_logits,
    reverse_forget_logits,
    output_gate_logits,
    onward_floor_gap,
    reverse_floor_gap,
    extra_log_decay,
    per_head_gain,
    residual,
    output_matrix,
    inner_norm_gain,
    inner_norm_bias,
    gate_matrix,
    up_matrix,
    down_matrix,
    closing_norm_gain,
    closing_norm_bias,
):
    weights = gathered_weights(gate_matrix, up_matrix, down_matrix)
    rows = query_logits.shape[0]
    inner, queries, packed = local_pass(
        query_logits,
        value_rows,
        onward_forget_logits,
        reverse_forget_logits,
        onward_floor_gap[None],
        reverse_floor_gap[None],
        extra_log_decay.reshape(1, rows),
    )
    packed, output_matrix, residual = lax.optimization_barrier((packed, output_matrix, residual))
    back = states_around(packed)
    blocks = spread_over_x(output_matrix, residual, inner_norm_gain, inner_norm_bias)
    gated = gated_rows(back, inner, queries, per_head_gain[None], output_gate_logits)
    everyone = lax.all_to_all(gated, ("yb", "x"), 0, 0, tiled=True)
    everyone = lax.all_gather(everyone, "c")
    both = []
    for block in blocks:
        both += [block, lax.ppermute(block, "c", SWAP)]
    middle, own = middle_rows(everyone, both)
    core = lax.axis_index("c").astype(jnp.int32)[None]
    send, hidden = feed_enter(core, middle, weights)
    other = lax.ppermute(send, "c", SWAP)
    mine = feed_leave(core, hidden, weights)
    shares = lax.all_to_all(joined(mine, other), ("yb", "x"), 0, 0, tiled=True)
    before_final, moments = pl.pallas_call(
        total_kernel,
        out_shape=[
            pltpu.VMEM(own.shape, jnp.float32),
            pltpu.VMEM((8, 1, 2 * rows), jnp.float32),
        ],
        compiler_params=pltpu.CompilerParams(vmem_limit_bytes=4 << 20),
        name="total",
    )(*near(shares, own))
    moments = lax.all_to_all(moments, TP, 0, 0, tiled=True)
    return pl.pallas_call(
        closing_kernel,
        out_shape=jax.ShapeDtypeStruct(own.shape, jnp.bfloat16),
        compiler_params=pltpu.CompilerParams(vmem_limit_bytes=4 << 20),
        name="closing",
    )(*near(moments, before_final, closing_norm_gain[None], closing_norm_bias[None]))


def solution(mesh):
    torus = Mesh(mesh.devices.reshape(8, 2, 2, 2, 4, 2), ("zb", "zr", "ya", "yb", "x", "c"))
    in_specs = (
        P(SP, TP),
        P(SP, TP),
        P(SP, TP),
        P(SP, TP),
        P(SP, TP),
        P(TP),
        P(TP),
        P(SP, TP),
        P(),
        P(SP, TP),
        P(None, TP),
        P(TP),
        P(TP),
        P(SP, TP),
        P(SP, TP),
        P(TP, SP),
        P(TP),
        P(TP),
    )
    out_specs = P(SP, TP)
    return jax.shard_map(layer, mesh=torus, in_specs=in_specs, out_specs=out_specs, check_vma=False)
```

```python
import jax
import jax.numpy as jnp
from jax import lax
from jax.experimental import pallas as pl
from jax.experimental.pallas import tpu as pltpu
from jax.sharding import Mesh
from jax.sharding import PartitionSpec as P


D = 2048
Z = ("zb", "zr")
NEAR = ("zr", "ya", "yb")
SP = ("zb", "zr", "ya", "yb")
TP = ("x", "c")
HALF = 352
SLICE = 16
BLOCK = 8

highest_precision = lax.Precision.HIGHEST
alpha_mix = 2.0**0.25
norm_eps = 1e-05
head_eps = 1e-06


def exact_dot(a, b, dims=((1,), (0,))):
    return lax.dot_general(
        a, b, (dims, ((), ())), precision=highest_precision, preferred_element_type=jnp.float32
    )


def two_terms(x):
    high = x.astype(jnp.bfloat16).astype(jnp.float32)
    return high, (x - high).astype(jnp.bfloat16).astype(jnp.float32)


def local_kernel(
    query_ref,
    value_ref,
    onward_ref,
    reverse_ref,
    onward_gap_ref,
    reverse_gap_ref,
    extra_ref,
    inner_ref,
    queries_ref,
    packed_ref,
    rows_ref,
):
    rows, width = query_ref.shape
    logits = query_ref[...].astype(jnp.float32)
    query = logits / (1.0 + jnp.exp(-logits))
    values = value_ref[...].astype(jnp.float32)
    extra = extra_ref[...]
    at = lax.broadcasted_iota(jnp.int32, (rows, rows), 0)
    source = lax.broadcasted_iota(jnp.int32, (rows, rows), 1)
    ones = jnp.ones((rows, width), jnp.float32)
    inner = jnp.zeros_like(query)
    rows_ref[:, 2 * SLICE :, :] = jnp.zeros((BLOCK, 8, width), jnp.float32)
    for side, (forget_ref, gap_ref, seen, last) in enumerate(
        (
            (onward_ref, onward_gap_ref, at >= source, rows - 1),
            (reverse_ref, reverse_gap_ref, at <= source, 0),
        )
    ):
        seen = seen.astype(jnp.float32)
        keys = gap_ref[...] / (1.0 + jnp.exp(forget_ref[...].astype(jnp.float32)))
        running = exact_dot(seen, jnp.log1p(-keys)) + exact_dot(seen * extra, ones)
        total = running[last : last + 1]
        decayed_query = query * jnp.exp(running)
        scores = exact_dot(decayed_query, keys * jnp.exp(-running), ((1,), (1,))) * seen
        inner = inner + exact_dot(scores, values)
        queries_ref[:, width * side : width * (side + 1)] = decayed_query
        state = exact_dot(values, keys * jnp.exp(total - running), ((0,), (0,)))
        terms = two_terms(total)
        for y in range(BLOCK):
            rows_ref[y, SLICE * side : SLICE * (side + 1), :] = state[
                SLICE * y : SLICE * (y + 1)
            ]
            for t in range(2):
                at_row = 2 * SLICE + 2 * side + t
                rows_ref[y, at_row : at_row + 1, :] = terms[t]
    packed_ref[...] = rows_ref[...].astype(jnp.bfloat16)
    inner_ref[...] = inner


def near(*arrays):
    return [pltpu.with_memory_space_constraint(a, pltpu.VMEM) for a in arrays]


def local_pass(*arrays):
    rows, width = arrays[0].shape
    return pl.pallas_call(
        local_kernel,
        out_shape=[
            pltpu.VMEM((rows, width), jnp.float32),
            pltpu.VMEM((rows, 2 * width), jnp.float32),
            pltpu.VMEM((BLOCK, 2 * SLICE + 8, width), jnp.bfloat16),
        ],
        scratch_shapes=[pltpu.VMEM((BLOCK, 2 * SLICE + 8, width), jnp.float32)],
        compiler_params=pltpu.CompilerParams(vmem_limit_bytes=6 << 20),
        name="local",
    )(*near(*arrays))


def plane_parts(arrived_ref):
    parts = []
    for side in range(2):
        part = []
        for y in range(BLOCK):
            block = arrived_ref[y].astype(jnp.float32)
            decay = block[2 * SLICE + 2 * side : 2 * SLICE + 2 * side + 1]
            decay = decay + block[2 * SLICE + 2 * side + 1 : 2 * SLICE + 2 * side + 2]
            part.append((decay, block[SLICE * side : SLICE * (side + 1)]))
        parts.append(part)
    return parts


def plane_kernel(z_ref, arrived_ref, out_ref, rows_ref):
    forward, backward = plane_parts(arrived_ref)
    wholes = []
    for part in (forward, backward[::-1]):
        decay, state = part[0]
        for next_decay, next_state in part[1:]:
            decay, state = decay + next_decay, jnp.exp(next_decay) * state + next_state
        wholes.append((decay, state))
    for side, (decay, state) in enumerate(wholes):
        rows_ref[side] = jnp.zeros(rows_ref.shape[1:], jnp.float32)
        rows_ref[side, :SLICE, :] = state
        for t, term in enumerate(two_terms(decay)):
            rows_ref[side, SLICE + t : SLICE + t + 1, :] = term
    ahead, behind = rows_ref[0].astype(jnp.bfloat16), rows_ref[1].astype(jnp.bfloat16)
    z = z_ref[0]
    for other in range(out_ref.shape[0]):

        @pl.when(other > z)
        def _():
            out_ref[other] = ahead

        @pl.when(other <= z)
        def _():
            out_ref[other] = behind


def before_kernel(z_ref, planes_ref, arrived_ref, out_ref):
    z = z_ref[0]
    planes = planes_ref.shape[0]
    width = planes_ref.shape[2]
    states = []
    for order in (range(planes), reversed(range(planes))):
        state = jnp.zeros((SLICE, width), jnp.float32)
        for other in order:
            block = planes_ref[other].astype(jnp.float32)
            decay = block[SLICE : SLICE + 1] + block[SLICE + 1 : SLICE + 2]
            passed = other < z if not states else other > z
            state = jnp.where(passed, jnp.exp(decay) * state + block[:SLICE], state)
        states.append(state)
    forward, backward = plane_parts(arrived_ref)
    for side, part in enumerate((forward, backward)):
        state = states[side]
        for y in range(BLOCK) if side == 0 else reversed(range(BLOCK)):
            out_ref[y, SLICE * side : SLICE * (side + 1)] = state.astype(jnp.bfloat16)
            decay, own = part[y]
            state = jnp.exp(decay) * state + own


def states_around(packed):
    z = lax.axis_index("zb").astype(jnp.int32)[None]
    planes = lax.axis_size("zb")
    width = packed.shape[2]
    (arrived,) = near(lax.all_to_all(packed, NEAR, 0, 0, tiled=True))
    totals = pl.pallas_call(
        plane_kernel,
        in_specs=[SMEM, VMEM],
        out_specs=VMEM,
        out_shape=pltpu.VMEM((planes, SLICE + 8, width), jnp.bfloat16),
        scratch_shapes=[pltpu.VMEM((2, SLICE + 8, width), jnp.float32)],
        compiler_params=pltpu.CompilerParams(vmem_limit_bytes=4 << 20),
        name="plane",
    )(z, arrived)
    (others,) = near(lax.all_to_all(totals, "zb", 0, 0, tiled=True))
    before = pl.pallas_call(
        before_kernel,
        in_specs=[SMEM, VMEM, VMEM],
        out_specs=VMEM,
        out_shape=pltpu.VMEM((BLOCK, 2 * SLICE, width), jnp.bfloat16),
        compiler_params=pltpu.CompilerParams(vmem_limit_bytes=4 << 20),
        name="before",
    )(z, others, arrived)
    return lax.all_to_all(before, NEAR, 0, 0, tiled=True)


def gated_kernel(back_ref, inner_ref, queries_ref, gain_ref, gate_ref, out_ref):
    width = inner_ref.shape[1]
    mixed = inner_ref[...]
    for side in range(2):
        state = [back_ref[y, SLICE * side : SLICE * (side + 1)] for y in range(BLOCK)]
        state = jnp.concatenate([part.astype(jnp.float32) for part in state], axis=0)
        queries = queries_ref[:, width * side : width * (side + 1)]
        mixed = mixed + exact_dot(queries, state, ((1,), (1,)))
    mean = jnp.mean(mixed * mixed, axis=1, keepdims=True)
    normed = mixed * lax.rsqrt(mean + head_eps) * gain_ref[...]
    gate = gate_ref[...].astype(jnp.float32)
    gated = (normed * (gate / (1.0 + jnp.exp(-gate)))).astype(jnp.bfloat16)
    for peer in range(out_ref.shape[0]):
        out_ref[peer] = gated


def gated_rows(*arrays):
    return pl.pallas_call(
        gated_kernel,
        out_shape=pltpu.VMEM((8, *arrays[1].shape), jnp.bfloat16),
        compiler_params=pltpu.CompilerParams(vmem_limit_bytes=4 << 20),
        name="gated",
    )(*near(*arrays))


SMEM = pl.BlockSpec(memory_space=pltpu.SMEM)
VMEM = pl.BlockSpec(memory_space=pltpu.VMEM)
ANY = pl.BlockSpec(memory_space=pl.ANY)


def turn_kernel(in_ref, out_ref):
    for kind in range(3):
        rows = jnp.concatenate([in_ref[y, kind] for y in range(4)], axis=0)
        out_ref[kind] = rows.T


def gathered_weights(gate, up, down):
    both = jnp.stack([gate, up, down.T])
    halves = [both[:, :, :HALF], both[:, :, HALF:]]
    arrived = lax.all_to_all(jnp.stack(halves + halves), ("ya", "yb"), 0, 0, tiled=True)
    shard = pl.pallas_call(
        turn_kernel,
        out_shape=jax.ShapeDtypeStruct((3, HALF, 128), jnp.bfloat16),
        compiler_params=pltpu.CompilerParams(vmem_limit_bytes=6 << 20),
        name="turn",
    )(*near(arrived)).reshape(3 * HALF, 128)
    weights = lax.all_gather(shard, Z, axis=0, tiled=True).reshape(-1, 3, HALF, 128)
    return pltpu.with_memory_space_constraint(weights, pltpu.HBM)


def exact_terms(x):
    terms = []
    for _ in range(3):
        term = lax.reduce_precision(x, 8, 7)
        terms.append(term.astype(jnp.bfloat16))
        x = x - term
    return terms


SWAP = ((0, 1), (1, 0))


def spread_over_x(output_matrix, residual, gain, bias):
    other = lax.ppermute(residual, "yb", SWAP)
    first = lax.axis_index("yb") == 0
    vectors = jnp.stack(exact_terms(gain) + exact_terms(bias))
    block = jnp.concatenate(
        [
            output_matrix,
            jnp.where(first, residual, other),
            jnp.where(first, other, residual),
            jnp.pad(vectors, ((0, 10), (0, 0))),
        ]
    )
    count = lax.axis_size("x")
    return [block] + [
        lax.ppermute(block, "x", [(i, (i + k) % count) for i in range(count)])
        for k in range(1, count)
    ]


def middle_kernel(place_ref, gated_ref, *refs):
    block_refs, (out_ref, own_ref, whole_ref, before_ref) = refs[:8], refs[8:]
    heads, rows = 8, gated_ref.shape[2]
    count = 2 * rows
    for core in range(2):
        for pair in range(2):
            for x in range(4):
                head = 2 * x + core
                whole_ref[pair * rows : (pair + 1) * rows, 128 * head : 128 * head + 128] = (
                    gated_ref[core, 4 * pair + x]
                )
    whole = whole_ref[...]
    inner = whole.shape[1]
    total = jnp.zeros((count, 1), jnp.float32)
    for b in range(heads):
        mixer = jnp.dot(whole, block_refs[b][:inner], preferred_element_type=jnp.float32)
        residual = block_refs[b][inner : inner + count].astype(jnp.float32)
        before = alpha_mix * residual + mixer
        before_ref[b] = before
        total = total + jnp.sum(before, axis=1, keepdims=True)
    mean = total / D
    spread = jnp.zeros((count, 1), jnp.float32)
    for b in range(heads):
        centre = before_ref[b] - mean
        spread = spread + jnp.sum(centre * centre, axis=1, keepdims=True)
    scale = lax.rsqrt(spread / D + norm_eps)
    for b in range(heads):
        vectors = block_refs[b][inner + count : inner + count + 16].astype(jnp.float32)
        gain = vectors[0:1] + vectors[1:2] + vectors[2:3]
        bias = vectors[3:4] + vectors[4:5] + vectors[5:6]
        normed = (before_ref[b] - mean) * scale * gain + bias
        normed = normed.astype(jnp.bfloat16)
        out_ref[place_ref[b]] = normed
        if b == 0:
            own_ref[...] = jnp.where(place_ref[heads] == 0, normed[:rows], normed[rows:])


def middle_rows(gated, blocks):
    rows, width = gated.shape[2], blocks[0].shape[1]
    x, core = lax.axis_index("x"), lax.axis_index("c")
    place = [2 * ((x - b // 2 + 4) % 4) + (core + b) % 2 for b in range(8)]
    place = jnp.stack(place + [lax.axis_index("yb")])
    vmem = pl.BlockSpec(memory_space=pltpu.VMEM)
    return pl.pallas_call(
        middle_kernel,
        in_specs=[pl.BlockSpec(memory_space=pltpu.SMEM)] + [vmem] * 9,
        out_specs=[vmem, vmem],
        out_shape=[
            pltpu.VMEM((8, 2 * rows, width), jnp.bfloat16),
            pltpu.VMEM((rows, width), jnp.bfloat16),
        ],
        scratch_shapes=[
            pltpu.VMEM((2 * rows, 8 * 128), jnp.bfloat16),
            pltpu.VMEM((8, 2 * rows, width), jnp.float32),
        ],
        compiler_params=pltpu.CompilerParams(vmem_limit_bytes=14 << 20),
        name="middle",
    )(place.astype(jnp.int32), *near(gated), *blocks)


def leaving(hidden, down_ref, block):
    wide = jnp.concatenate([down_ref[2 * block], down_ref[2 * block + 1]], axis=1)
    return jnp.dot(hidden, wide, preferred_element_type=jnp.float32)


def down_copies(core, weights_ref, leave_ref, sem_ref):
    copies = []
    for s in range(4):
        copies.append(
            pltpu.make_async_copy(
                weights_ref.at[pl.ds(4 * s + 2 * core, 2), 2],
                leave_ref.at[pl.ds(2 * s, 2)],
                sem_ref.at[s],
            )
        )
    return copies


def enter_kernel(
    core_ref, rows_ref, weights_ref, send_ref, hidden_ref, enter_ref, leave_ref, enter_sem, leave_sem
):
    parts, each = 4, 4
    copies = []
    for s in range(parts):
        copies.append(
            pltpu.make_async_copy(
                weights_ref.at[pl.ds(s * each, each), pl.ds(0, 2)],
                enter_ref.at[pl.ds(s * each, each)],
                enter_sem.at[s],
            )
        )
    downs = down_copies(1 - core_ref[0], weights_ref, leave_ref, leave_sem)
    for copy in copies:
        copy.start()
    sums = [0.0, 0.0]
    for s in range(parts):
        x = jnp.concatenate([rows_ref[2 * s], rows_ref[2 * s + 1]], axis=1)
        copies[s].wait()
        if s == 0:
            for copy in downs:
                copy.start()
        for kind in range(2):
            wide = [enter_ref[each * s + j, kind] for j in range(each)]
            sums[kind] += lax.dot_general(
                x,
                jnp.concatenate(wide, axis=1),
                (((1,), (1,)), ((), ())),
                preferred_element_type=jnp.float32,
            )
    gate, up = sums
    hidden = (gate / (1.0 + jnp.exp(-gate)) * up).astype(jnp.bfloat16)
    hidden_ref[...] = hidden
    rows = send_ref.shape[2]
    for s in range(4):
        downs[s].wait()
        product = leaving(hidden, leave_ref, s).astype(jnp.bfloat16)
        send_ref[0, s] = product[:rows]
        send_ref[1, s] = product[rows:]


def leave_kernel(core_ref, hidden_ref, weights_ref, out_ref, leave_ref, leave_sem):
    downs = down_copies(core_ref[0], weights_ref, leave_ref, leave_sem)
    for copy in downs:
        copy.start()
    hidden = hidden_ref[...]
    rows = out_ref.shape[2]
    for s in range(4):
        downs[s].wait()
        product = leaving(hidden, leave_ref, s)
        out_ref[0, s] = product[:rows]
        out_ref[1, s] = product[rows:]


def join_kernel(mine_ref, other_ref, out_ref):
    for pair in range(2):
        for s in range(4):
            total = mine_ref[pair, s] + other_ref[pair, s].astype(jnp.float32)
            out_ref[4 * pair + s] = total.astype(jnp.bfloat16)


def feed_enter(core, rows, weights):
    blocks, count, width = rows.shape
    return pl.pallas_call(
        enter_kernel,
        in_specs=[SMEM, VMEM, ANY],
        out_specs=[VMEM, VMEM],
        out_shape=[
            pltpu.VMEM((2, blocks // 2, count // 2, width), jnp.bfloat16),
            pltpu.VMEM((count, HALF), jnp.bfloat16),
        ],
        scratch_shapes=[
            pltpu.VMEM((16, 2, HALF, 128), jnp.bfloat16),
            pltpu.VMEM((8, HALF, 128), jnp.bfloat16),
            pltpu.SemaphoreType.DMA((4,)),
            pltpu.SemaphoreType.DMA((4,)),
        ],
        cost_estimate=pl.CostEstimate(
            flops=5 * count * D * HALF, bytes_accessed=5 * D * HALF, transcendentals=count * HALF
        ),
        compiler_params=pltpu.CompilerParams(vmem_limit_bytes=16 << 20),
        name="feed_enter",
    )(core, *near(rows), weights)


def feed_leave(core, hidden, weights):
    count = hidden.shape[0]
    return pl.pallas_call(
        leave_kernel,
        in_specs=[SMEM, VMEM, ANY],
        out_specs=VMEM,
        out_shape=pltpu.VMEM((2, 4, count // 2, 256), jnp.float32),
        scratch_shapes=[
            pltpu.VMEM((8, HALF, 128), jnp.bfloat16),
            pltpu.SemaphoreType.DMA((4,)),
        ],
        cost_estimate=pl.CostEstimate(
            flops=count * D * HALF, bytes_accessed=D * HALF, transcendentals=0
        ),
        compiler_params=pltpu.CompilerParams(vmem_limit_bytes=8 << 20),
        name="feed_leave",
    )(core, *near(hidden), weights)


def joined(mine, other):
    return pl.pallas_call(
        join_kernel,
        out_shape=pltpu.VMEM((8, *mine.shape[2:]), jnp.bfloat16),
        compiler_params=pltpu.CompilerParams(vmem_limit_bytes=8 << 20),
        name="join",
    )(*near(mine, other))


def diagonal_of(rows):
    at = lax.broadcasted_iota(jnp.int32, (rows, rows), 0)
    return (at == lax.broadcasted_iota(jnp.int32, (rows, rows), 1)).astype(jnp.float32)


def total_kernel(arrived_ref, own_ref, before_ref, moments_ref):
    feed = arrived_ref[0].astype(jnp.float32)
    for peer in range(1, arrived_ref.shape[0]):
        feed = feed + arrived_ref[peer].astype(jnp.float32)
    before = alpha_mix * own_ref[...].astype(jnp.float32) + feed
    before_ref[...] = before
    diagonal = diagonal_of(before.shape[0])
    moments = []
    for value in (before, before * before):
        column = jnp.sum(value, axis=1, keepdims=True)
        moments.append(jnp.sum(diagonal * column, axis=0, keepdims=True))
    moments = jnp.concatenate(moments, axis=1)
    for peer in range(moments_ref.shape[0]):
        moments_ref[peer] = moments


def closing_kernel(moments_ref, before_ref, gain_ref, bias_ref, out_ref):
    moments = moments_ref[0]
    for peer in range(1, moments_ref.shape[0]):
        moments = moments + moments_ref[peer]
    rows = before_ref.shape[0]
    mean = moments[:, :rows] / D
    spread = moments[:, rows:] / D - mean * mean
    diagonal = diagonal_of(rows)
    column = jnp.sum(diagonal * mean, axis=1, keepdims=True)
    factor = jnp.sum(diagonal * lax.rsqrt(spread + norm_eps), axis=1, keepdims=True)
    out_ref[...] = ((before_ref[...] - column) * factor * gain_ref[...] + bias_ref[...]).astype(
        jnp.bfloat16
    )


def layer(
    query_logits,
    value_rows,
    onward_forget_logits,
    reverse_forget_logits,
    output_gate_logits,
    onward_floor_gap,
    reverse_floor_gap,
    extra_log_decay,
    per_head_gain,
    residual,
    output_matrix,
    inner_norm_gain,
    inner_norm_bias,
    gate_matrix,
    up_matrix,
    down_matrix,
    closing_norm_gain,
    closing_norm_bias,
):
    weights = gathered_weights(gate_matrix, up_matrix, down_matrix)
    rows = query_logits.shape[0]
    inner, queries, packed = local_pass(
        query_logits,
        value_rows,
        onward_forget_logits,
        reverse_forget_logits,
        onward_floor_gap[None],
        reverse_floor_gap[None],
        extra_log_decay.reshape(1, rows),
    )
    packed, output_matrix, residual = lax.optimization_barrier((packed, output_matrix, residual))
    back = states_around(packed)
    blocks = spread_over_x(output_matrix, residual, inner_norm_gain, inner_norm_bias)
    gated = gated_rows(back, inner, queries, per_head_gain[None], output_gate_logits)
    everyone = lax.all_to_all(gated, ("yb", "x"), 0, 0, tiled=True)
    everyone = lax.all_gather(everyone, "c")
    both = []
    for block in blocks:
        both += [block, lax.ppermute(block, "c", SWAP)]
    middle, own = middle_rows(everyone, both)
    core = lax.axis_index("c").astype(jnp.int32)[None]
    send, hidden = feed_enter(core, middle, weights)
    other = lax.ppermute(send, "c", SWAP)
    mine = feed_leave(core, hidden, weights)
    shares = lax.all_to_all(joined(mine, other), ("yb", "x"), 0, 0, tiled=True)
    before_final, moments = pl.pallas_call(
        total_kernel,
        out_shape=[
            pltpu.VMEM(own.shape, jnp.float32),
            pltpu.VMEM((8, 1, 2 * rows), jnp.float32),
        ],
        compiler_params=pltpu.CompilerParams(vmem_limit_bytes=4 << 20),
        name="total",
    )(*near(shares, own))
    moments = lax.all_to_all(moments, TP, 0, 0, tiled=True)
    return pl.pallas_call(
        closing_kernel,
        out_shape=jax.ShapeDtypeStruct(own.shape, jnp.bfloat16),
        compiler_params=pltpu.CompilerParams(vmem_limit_bytes=4 << 20),
        name="closing",
    )(*near(moments, before_final, closing_norm_gain[None], closing_norm_bias[None]))


def solution(mesh):
    torus = Mesh(mesh.devices.reshape(8, 2, 2, 2, 4, 2), ("zb", "zr", "ya", "yb", "x", "c"))
    in_specs = (
        P(SP, TP),
        P(SP, TP),
        P(SP, TP),
        P(SP, TP),
        P(SP, TP),
        P(TP),
        P(TP),
        P(SP, TP),
        P(),
        P(SP, TP),
        P(None, TP),
        P(TP),
        P(TP),
        P(SP, TP),
        P(SP, TP),
        P(TP, SP),
        P(TP),
        P(TP),
    )
    out_specs = P(SP, TP)
    return jax.shard_map(layer, mesh=torus, in_specs=in_specs, out_specs=out_specs, check_vma=False)
```
